128 devices in a mesh: ep: 128 (over z, y, x, core).
Axes of the slice: x: 4, y: 4, z: 4, core: 2. Of those that a mesh axis runs over, the one named last changes fastest.
Arguments:
- tokens: bfloat16 [128, 2048], P('ep'), may hold values from -6 to 6
- mixer_gain: float32 [2048], replicated, may hold values from 0.1 to 1.9
- query_weight: bfloat16 [2048, 2048], P(None, 'ep'), may hold values from -0.125 to 0.125
- key_weight: bfloat16 [2048, 2048], P(None, 'ep'), may hold values from -0.125 to 0.125
- value_weight: bfloat16 [2048, 2048], P(None, 'ep'), may hold values from -0.125 to 0.125
- outgate_weight: bfloat16 [2048, 2048], P(None, 'ep'), may hold values from -0.125 to 0.125
- input_weight: bfloat16 [2048, 4], replicated, may hold values from -0.125 to 0.125
- forget_weight: bfloat16 [2048, 4], replicated, may hold values from -0.125 to 0.125
- forget_bias: float32 [4], replicated, may hold values from 0 to 4
- memory_matrix: float32 [128, 4, 512, 512], P('ep'), may hold values from -0.3 to 0.3
- memory_norm: float32 [128, 4, 512], P('ep'), may hold values from -0.3 to 0.3
- memory_max: float32 [128, 4], P('ep'), may hold values from -2 to 2
- mixer_out: bfloat16 [2048, 2048], P(None, 'ep'), may hold values from -0.125 to 0.125
- expert_gain: float32 [2048], replicated, may hold values from 0.1 to 1.9
- expert_gate: bfloat16 [128, 2048, 1024], P('ep'), may hold values from -0.125 to 0.125
- expert_up: bfloat16 [128, 2048, 1024], P('ep'), may hold values from -0.125 to 0.125
- expert_down: bfloat16 [128, 1024, 2048], P('ep'), may hold values from -0.1875 to 0.1875
- route_group: int32 [128], P('ep'), may hold values from 0 to 3
- route_member: int32 [128, 2], P('ep'), may hold values from 0 to 31, as said below
- group_weight: float32 [128], P('ep'), may hold values from 0.25 to 1
- member_weight: float32 [128, 2], P('ep'), may hold values from 0.1 to 1
Outputs:
- layer_out: bfloat16 [128, 2048], P('ep')
- next_matrix: float32 [128, 4, 512, 512], P('ep')
- next_norm: float32 [128, 4, 512], P('ep')
- next_max: float32 [128, 4], P('ep')
The draws below stay inside these ranges and needn't reach their ends.
Inputs may be any that keep to these rules, and one draw needn't show every extreme that they name: A row's 2 experts, numbered route_group * 32 + route_member, are different members of the one group that route_group names. No expert is named by more than 4 rows in all, and one expert is named by exactly 4 rows.
All inputs are finite; a program needn't handle non-finite values.
Results may differ from the reference program's by a relative error of at most 0.013.
Values may be sent and summed in bfloat16 or wider, within the bound.
A program may use at most 64 MiB of HBM per device.

```python
import math
import jax
import jax.numpy as jnp
from jax import lax

D = 2048
HEADS = 4
HEAD_DIM = 512
FF = 1024
GROUPS = 4
TOP_K = 2
SEQ_DEV = 1
TOKENS = 128
EXPERTS = 128
MEMBERS = 32
CAPACITY = 4


def route_tables(key):
    base = jax.random.fold_in(key, 11)
    streams = jax.random.split(base, 4)
    favour = jax.random.randint(streams[0], (EXPERTS,), 0, 64)
    hottest = jax.random.randint(streams[1], (), 0, EXPERTS)
    noise = jax.random.randint(streams[2], (TOKENS, EXPERTS), 0, 64)
    column = jnp.arange(EXPERTS, dtype=jnp.int32)
    row_index = jnp.arange(TOKENS, dtype=jnp.int32)
    score = noise + 2 * favour[None, :] + jnp.where(column == hottest, 4096, 0)[None, :]
    forced = jnp.where((row_index[:, None] == 0) & (column[None, :] == EXPERTS // 2), 16384, 0)
    forced = forced + jnp.where((row_index[:, None] == SEQ_DEV) & (column[None, :] == 0), 16384, 0)
    score = (score + forced) * EXPERTS + column[None, :]
    ranking = jax.random.permutation(streams[3], TOKENS).astype(jnp.int32)
    ranking = jnp.where(row_index == 0, -2, jnp.where(row_index == SEQ_DEV, -1, ranking))
    order = jnp.argsort(ranking).astype(jnp.int32)

    def visit(load, row):
        open_slots = load < CAPACITY
        masked = jnp.where(open_slots, score[row], -1)
        counts = jnp.sum(open_slots.reshape(GROUPS, MEMBERS).astype(jnp.int32), axis=1)
        best = jnp.where(counts >= TOP_K, jnp.max(masked.reshape(GROUPS, MEMBERS), axis=1), -1 - jnp.arange(GROUPS, dtype=jnp.int32))
        group_pick = lax.top_k(best, 1)[1][0].astype(jnp.int32)
        inside = lax.dynamic_slice_in_dim(masked, group_pick * MEMBERS, MEMBERS)
        picks = lax.top_k(inside, TOP_K)[1].astype(jnp.int32)
        load = load.at[group_pick * MEMBERS + picks].add(1)
        return (load, (group_pick, picks))
    _, (groups_seen, members_seen) = lax.scan(visit, jnp.zeros((EXPERTS,), jnp.int32), order)
    group_ids = jnp.zeros((TOKENS,), jnp.int32).at[order].set(groups_seen)
    member_ids = jnp.zeros((TOKENS, TOP_K), jnp.int32).at[order].set(members_seen)
    return (group_ids, member_ids)


def draw_route_group(key, part):
    return route_tables(key)[0]


def draw_route_member(key, part):
    return route_tables(key)[1]


def steps_of(key, shape, pieces, smallest, top_value):
    def one(position, blocks):
        steps = jax.random.uniform(jax.random.fold_in(jax.random.fold_in(key, 6), position), (blocks,), jnp.float32, smallest / len(pieces), top_value / len(pieces))
        return jnp.repeat(jnp.exp(steps), shape[position] // blocks).reshape((-1,) + (1,) * (len(shape) - position - 1))

    loudness = one(*pieces[0])
    for cut in pieces[1:]:
        loudness = loudness * one(*cut)
    return loudness


def scatter_about(rng, extent, width, reach, cuts=(), kind=jnp.bfloat16):
    level = steps_of(rng, extent, cuts, -0.22, 0.18) if cuts else 1.0
    drawn = jax.random.normal(rng, extent, jnp.float32) * width * level
    return jnp.minimum(jnp.maximum(drawn, -reach), reach).astype(kind)


def setup_inputs(seed: int = 0) -> dict:
    arg_keys = jax.random.split(jax.random.key(seed), 22)
    return {
        "tokens": scatter_about(arg_keys[0], (TOKENS, D), 1.0, 6.0, ((0, 128),)),
        "mixer_gain": jnp.clip(1.0 + 0.18 * jax.random.normal(arg_keys[1], (D,), jnp.float32), 0.1, 1.9),
        "query_weight": scatter_about(arg_keys[2], (D, D), D ** -0.5, 0.125, ((1, 128),)),
        "key_weight": scatter_about(arg_keys[3], (D, D), D ** -0.5, 0.125, ((1, 128),)),
        "value_weight": scatter_about(arg_keys[4], (D, D), D ** -0.5, 0.125, ((1, 128),)),
        "outgate_weight": scatter_about(arg_keys[5], (D, D), D ** -0.5, 0.125, ((1, 128),)),
        "input_weight": scatter_about(arg_keys[6], (D, HEADS), D ** -0.5, 0.125),
        "forget_weight": scatter_about(arg_keys[7], (D, HEADS), D ** -0.5, 0.125),
        "forget_bias": jnp.clip(jax.random.uniform(arg_keys[8], (HEADS,), jnp.float32, 0.0, 4.0), 0.0, 4.0),
        "memory_matrix": scatter_about(arg_keys[9], (TOKENS, HEADS, HEAD_DIM, HEAD_DIM), 0.05, 0.3, ((0, 128),), jnp.float32),
        "memory_norm": scatter_about(arg_keys[10], (TOKENS, HEADS, HEAD_DIM), 0.05, 0.3, ((0, 128),), jnp.float32),
        "memory_max": jnp.clip(jax.random.uniform(arg_keys[11], (TOKENS, HEADS), jnp.float32, -2.0, 2.0) * steps_of(arg_keys[11], (TOKENS, HEADS), ((0, 128),), -0.4, 0.0), -2.0, 2.0),
        "mixer_out": scatter_about(arg_keys[12], (D, D), D ** -0.5, 0.125, ((1, 128),)),
        "expert_gain": jnp.clip(1.0 + 0.18 * jax.random.normal(arg_keys[13], (D,), jnp.float32), 0.1, 1.9),
        "expert_gate": scatter_about(arg_keys[14], (EXPERTS, D, FF), D ** -0.5, 0.125, ((0, 128),)),
        "expert_up": scatter_about(arg_keys[15], (EXPERTS, D, FF), D ** -0.5, 0.125, ((0, 128),)),
        "expert_down": scatter_about(arg_keys[16], (EXPERTS, FF, D), FF ** -0.5, 0.1875, ((0, 128),)),
        "route_group": draw_route_group(jax.random.fold_in(arg_keys[21], 71), 0),
        "route_member": draw_route_member(jax.random.fold_in(arg_keys[21], 71), 0),
        "group_weight": jnp.clip(jnp.exp(math.log(1.0) - 1.3862944 * jax.random.uniform(arg_keys[19], (TOKENS,), jnp.float32) ** steps_of(arg_keys[19], (TOKENS,), ((0, 128),), -0.2, 0.2)), 0.25, 1.0),
        "member_weight": jnp.clip(jnp.exp(math.log(1.0) - 2.3025851 * jax.random.uniform(arg_keys[20], (TOKENS, TOP_K), jnp.float32) ** steps_of(arg_keys[20], (TOKENS, TOP_K), ((0, 128),), -0.2, 0.2)), 0.1, 1.0),
    }


norm_eps = 1e-06

def root_norm(values, gain):
    return values * lax.rsqrt(lax.optimization_barrier(jnp.mean(values * values, axis=-1, keepdims=True)) + norm_eps) * gain

def reference(tokens, mixer_gain, query_weight, key_weight, value_weight, outgate_weight, input_weight, forget_weight, forget_bias, memory_matrix, memory_norm, memory_max, mixer_out, expert_gain, expert_gate, expert_up, expert_down, route_group, route_member, group_weight, member_weight):
    count = tokens.shape[0]
    resid = tokens.astype(jnp.float32)
    normed = root_norm(resid, mixer_gain).astype(jnp.bfloat16)
    query = jnp.dot(normed, query_weight, preferred_element_type=jnp.float32).astype(jnp.bfloat16)
    key = jnp.dot(normed, key_weight, preferred_element_type=jnp.float32).astype(jnp.bfloat16)
    value = jnp.dot(normed, value_weight, preferred_element_type=jnp.float32).astype(jnp.bfloat16)
    outgate = jnp.dot(normed, outgate_weight, preferred_element_type=jnp.float32).astype(jnp.bfloat16)
    input_pre = jnp.dot(normed, input_weight, preferred_element_type=jnp.float32)
    forget_pre = jnp.dot(normed, forget_weight, preferred_element_type=jnp.float32) + forget_bias
    log_forget = jax.nn.log_sigmoid(forget_pre)
    next_max = jnp.maximum(log_forget + memory_max, input_pre)
    keep = jnp.exp(log_forget + memory_max - next_max)
    admit = jnp.exp(input_pre - next_max)
    query_heads = query.astype(jnp.float32).reshape(count, HEADS, HEAD_DIM)
    key_heads = key.astype(jnp.float32).reshape(count, HEADS, HEAD_DIM) * HEAD_DIM ** (-0.5)
    value_heads = value.astype(jnp.float32).reshape(count, HEADS, HEAD_DIM)
    carried = jnp.einsum('shij,shj->shi', memory_matrix, query_heads, precision=lax.Precision.HIGHEST)
    score = lax.optimization_barrier(jnp.sum(key_heads * query_heads, axis=-1))
    numer = keep[..., None] * carried + (admit * score)[..., None] * value_heads
    denom = keep * lax.optimization_barrier(jnp.sum(memory_norm * query_heads, axis=-1)) + admit * score
    head_out = numer / jnp.maximum(jnp.abs(denom), jnp.exp(-next_max))[..., None]
    gated = (head_out.reshape(count, D) * jax.nn.sigmoid(outgate.astype(jnp.float32))).astype(jnp.bfloat16)
    next_matrix = keep[..., None, None] * memory_matrix + admit[..., None, None] * value_heads[..., :, None] * key_heads[..., None, :]
    next_norm = keep[..., None] * memory_norm + admit[..., None] * key_heads
    projected = jnp.dot(gated, mixer_out, preferred_element_type=jnp.float32).astype(jnp.bfloat16)
    middle = (resid + projected.astype(jnp.float32)).astype(jnp.bfloat16)
    expert_in = root_norm(middle.astype(jnp.float32), expert_gain).astype(jnp.bfloat16)
    chosen = (route_group[:, None] * MEMBERS + route_member).astype(jnp.int32)
    slot_rows = jnp.repeat(jnp.arange(count, dtype=jnp.int32), TOP_K)

    def one_slot(pair):
        row_index, expert_index = pair
        row = lax.dynamic_slice_in_dim(expert_in, row_index, 1, 0)
        gate_part = jnp.dot(row, expert_gate[expert_index], preferred_element_type=jnp.float32)
        up_part = jnp.dot(row, expert_up[expert_index], preferred_element_type=jnp.float32)
        hidden = (jax.nn.silu(gate_part) * up_part).astype(jnp.bfloat16)
        return jnp.dot(hidden, expert_down[expert_index], preferred_element_type=jnp.float32).astype(jnp.bfloat16)[0]
    results = lax.map(one_slot, (slot_rows, chosen.reshape(-1))).reshape(count, TOP_K, D)
    weight = group_weight[:, None] * member_weight
    mixture = lax.optimization_barrier(jnp.sum(weight[..., None] * results.astype(jnp.float32), axis=1))
    layer_out = (middle.astype(jnp.float32) + mixture).astype(jnp.bfloat16)
    return (layer_out, next_matrix, next_norm, next_max)
```

```python
import functools

import jax
import jax.numpy as jnp
from jax import lax
from jax.experimental import pallas as pl
from jax.experimental.pallas import tpu as pltpu
from jax.sharding import PartitionSpec as P

MESH = pl.DeviceIdType.MESH
F32 = jnp.float32
BF16 = jnp.bfloat16
EPS = 1e-06
CHIPS = 64
TILE = 16
LANES = 128
MEMBERS = 32


def nt(a, b):
    return lax.dot_general(a, b, (((1,), (1,)), ((), ())), preferred_element_type=F32)


def nn(a, b):
    return lax.dot_general(a, b, (((1,), (0,)), ((), ())), preferred_element_type=F32)


def tn(a, b):
    return lax.dot_general(a, b, (((0,), (0,)), ((), ())), preferred_element_type=F32)


def iota(shape, dim):
    return lax.broadcasted_iota(jnp.int32, shape, dim)


def pieces(row):
    return [row[:, LANES * s : LANES * (s + 1)] for s in range(row.shape[1] // LANES)]


def layer(
    tokens,
    mixer_gain,
    wq,
    wk,
    wv,
    wo,
    wi,
    wf,
    forget_bias,
    memory,
    memory_norm,
    memory_max,
    wm,
    expert_gain,
    gate,
    up,
    down,
    route_group,
    route_member,
    group_weight,
    member_weight,
    out_ref,
    next_memory,
    next_norm,
    next_max_ref,
    w_all,
    mem,
    mem16,
    gate_v,
    up_v,
    down_v,
    spread,
    perm,
    rows32,
    tok_rows,
    tile32,
    a_buf,
    b_src,
    b_buf,
    c_buf,
    p_buf,
    f_src,
    f_buf,
    e_rows,
    x_rows,
    r_rows,
    r_send,
    send_sem,
    recv_sem,
    load_sem,
    w_sem,
    out_sem,
    pair_sem,
):
    me = lax.axis_index("ep")
    core = lax.rem(me, 2)
    chip = lax.div(me, 2)
    other = 1 - core
    partner = me + 1 - 2 * core
    cz, cy, cx = lax.div(chip, 16), lax.rem(lax.div(chip, 4), 4), lax.rem(chip, 4)

    def peer(i):
        dz, dy, dx = lax.div(i, 16), lax.rem(lax.div(i, 4), 4), lax.rem(i, 4)
        there = lax.rem(cz + dz, 4) * 16 + lax.rem(cy + dy, 4) * 4 + lax.rem(cx + dx, 4)
        return there, there * 2 + core

    barrier = pltpu.get_barrier_semaphore()

    def greet(i, carry):
        pl.semaphore_signal(barrier, inc=1, device_id=(peer(i)[1],), device_id_type=MESH)
        return carry

    lax.fori_loop(1, CHIPS, greet, 0)
    pl.semaphore_signal(barrier, inc=1, device_id=(partner,), device_id_type=MESH)

    own_loads = []
    for j, ref in enumerate((wq, wk, wv, wo, wm)):
        own_loads.append(pltpu.make_async_copy(ref, w_all.at[j, core], w_sem.at[j]))
    mem_load = pltpu.make_async_copy(memory, mem, load_sem.at[0])
    gate_loads = [pltpu.make_async_copy(gate.at[:, u], gate_v.at[u], load_sem.at[1 + u]) for u in range(2)]
    up_loads = [pltpu.make_async_copy(up.at[:, u], up_v.at[u], load_sem.at[3 + u]) for u in range(2)]
    down_load = pltpu.make_async_copy(down, down_v, load_sem.at[5])
    for load in own_loads + [mem_load] + gate_loads + up_loads + [down_load]:
        load.start()

    def exchange(phase, source, buf):
        def send(n, carry):
            there, device = peer(CHIPS - n)
            pltpu.make_async_remote_copy(
                src_ref=source(there),
                dst_ref=buf.at[chip],
                send_sem=send_sem.at[phase],
                recv_sem=recv_sem.at[phase],
                device_id=(device,),
                device_id_type=MESH,
            ).start()
            return carry

        lax.fori_loop(1, CHIPS, send, 0)

    def whole(phase, buf):
        span = buf.at[pl.ds(0, CHIPS - 1)]
        return pltpu.make_async_remote_copy(
            src_ref=span,
            dst_ref=span,
            send_sem=send_sem.at[phase],
            recv_sem=recv_sem.at[phase],
            device_id=(partner,),
            device_id_type=MESH,
        )

    token = tokens[...].astype(F32)
    for s, piece in enumerate(pieces(token)):
        tile32[s : s + 1, :] = piece
    a_buf[chip] = tile32[...].astype(BF16)

    pl.semaphore_wait(barrier, CHIPS)

    exchange(0, lambda there: a_buf.at[chip], a_buf)
    swaps = []
    for j, ref in enumerate((wq, wk, wv, wo, wm)):
        swaps.append(
            pltpu.make_async_remote_copy(
                src_ref=ref,
                dst_ref=w_all.at[j, core],
                send_sem=pair_sem.at[0, j],
                recv_sem=pair_sem.at[1, j],
                device_id=(partner,),
                device_id_type=MESH,
            )
        )
        swaps[j].start()

    gain = mixer_gain[...]
    scale = lax.rsqrt(jnp.mean(token * token, axis=-1, keepdims=True) + EPS)
    normed = (token * scale * gain).astype(BF16).astype(F32)
    head_of = iota((4, 1), 0)

    def column(read):
        value = jnp.zeros((4, 1), F32)
        for h in range(4):
            value = jnp.where(head_of == h, read(h), value)
        return value

    input_pre = jnp.sum(wi[...].astype(F32) * normed, axis=1, keepdims=True)
    forget_pre = jnp.sum(wf[...].astype(F32) * normed, axis=1, keepdims=True) + column(lambda h: forget_bias[h])
    log_forget = jnp.minimum(forget_pre, 0.0) - jnp.log1p(jnp.exp(-jnp.abs(forget_pre)))
    held = log_forget + column(lambda h: memory_max[0, h])
    next_max = jnp.maximum(held, input_pre)
    keep = jnp.exp(held - next_max)
    admit = jnp.exp(input_pre - next_max)
    next_max_ref[...] = jnp.sum(
        jnp.where(iota((4, 4), 0) == iota((4, 4), 1), jnp.broadcast_to(next_max, (4, 4)), 0.0), axis=0, keepdims=True
    )

    lane = iota((1, LANES), 1)
    e0 = (route_group[0] * MEMBERS + route_member[0, 0]).astype(F32)
    e1 = (route_group[0] * MEMBERS + route_member[0, 1]).astype(F32)
    w0 = group_weight[0] * member_weight[0, 0]
    w1 = group_weight[0] * member_weight[0, 1]
    routing = jnp.where(lane == 0, e0, jnp.where(lane == 1, e1, jnp.where(lane == 2, w0, jnp.where(lane == 3, w1, 0.0))))
    b_src[:, 1:2, :] = jnp.broadcast_to(routing[None], (CHIPS, 1, LANES))

    for j in range(4):
        a, b = iota((LANES, 512), 0), iota((LANES, 512), 1)
        spread[:, 512 * j : 512 * (j + 1)] = (a == 32 * j + lax.rem(b, 32)).astype(F32).astype(BF16)
    a, b = iota((256, 256), 0), iota((256, 256), 1)
    perm[...] = (b == 128 * lax.rem(lax.div(a, 16), 2) + 16 * lax.div(a, 32) + lax.rem(a, 16)).astype(F32).astype(BF16)

    def reorder(rows):
        q = perm[...]
        parts = [nn(rows[:, 256 * m : 256 * (m + 1)], q) for m in range(8)]
        return jnp.concatenate([p[:, :LANES] for p in parts] + [p[:, LANES:] for p in parts], axis=1)

    def restore(rows):
        q = perm[...]
        parts = [
            nt(jnp.concatenate([rows[:, LANES * m : LANES * (m + 1)], rows[:, 1024 + LANES * m : 1024 + LANES * (m + 1)]], axis=1), q)
            for m in range(8)
        ]
        return jnp.concatenate(parts, axis=1)

    g = expert_gain[...]
    g_hi = g.astype(BF16)
    g_mid = (g - g_hi.astype(F32)).astype(BF16)
    g_lo = (g - g_hi.astype(F32) - g_mid.astype(F32)).astype(BF16)
    late_gain = jnp.zeros((1, 2048), F32)
    for part in (g_hi, g_mid, g_lo):
        late_gain = late_gain + reorder(jnp.broadcast_to(part.astype(F32), (16, 2048)).astype(BF16))[0:1]

    mem_load.wait()
    for h in range(4):
        mem16[h] = mem[h].astype(BF16)
    for load in own_loads:
        load.wait()
    for swap in swaps:
        swap.wait_recv()

    def gathered(buf):
        rows32[...] = buf[...].astype(F32).reshape(CHIPS * TILE, LANES)
        return [rows32[pl.ds(s, CHIPS, stride=TILE), :] for s in range(TILE)]

    whole(0, a_buf).wait_recv()
    parts = gathered(a_buf)
    tok_rows[...] = jnp.concatenate([p.astype(BF16) for p in parts], axis=1)
    squares = parts[0] * parts[0]
    for p in parts[1:]:
        squares = squares + p * p
    scale = lax.rsqrt(jnp.sum(squares, axis=-1, keepdims=True) * (1.0 / 2048.0) + EPS)
    normed_rows = jnp.concatenate(
        [(p * scale * gain[:, LANES * s : LANES * (s + 1)]).astype(BF16) for s, p in enumerate(parts)], axis=1
    )
    cols = nt(normed_rows, w_all[0:4].reshape(LANES, 2048)).astype(BF16).astype(F32)
    b_src[:, 0:1, :] = cols.reshape(CHIPS, 1, LANES)
    exchange(1, lambda there: b_src.at[there], b_buf)
    b_buf[chip] = b_src[chip]

    whole(1, b_buf).wait_recv()
    got = b_buf[:, 0:1, :].reshape(CHIPS, LANES).astype(BF16)
    wide = nn(got, spread[...])
    mine = lax.div(lax.rem(iota((CHIPS, 2048), 1), 512), 32) == lax.rem(iota((CHIPS, 2048), 0), 16)
    wide = jnp.where(mine, wide, 0.0).astype(BF16)
    heads = (iota((16, CHIPS), 0) == lax.div(iota((16, CHIPS), 1), 16)).astype(F32).astype(BF16)
    packed = nn(heads, wide)[0:4]
    query, key_raw, value, outgate = (packed[:, 512 * j : 512 * (j + 1)] for j in range(4))
    key = key_raw * (512.0**-0.5)
    score = jnp.sum(key * query, axis=-1, keepdims=True)
    old_norm = memory_norm[0]
    denom = keep * jnp.sum(old_norm * query, axis=-1, keepdims=True) + admit * score
    query16 = query.astype(BF16)
    head_row = iota((4, 512), 0)
    carried = jnp.zeros((4, 512), F32)
    for h in range(4):
        carried = jnp.where(head_row == h, nt(query16, mem16[h]), carried)
    numer = keep * carried + (admit * score) * value
    head_out = numer / jnp.maximum(jnp.abs(denom), jnp.exp(-next_max))
    gated = head_out * jax.nn.sigmoid(outgate)
    for b in range(4):
        tile32[pl.ds(b, 4, stride=4), :] = gated[:, LANES * b : LANES * (b + 1)]
    c_buf[chip] = tile32[...].astype(BF16)
    exchange(2, lambda there: c_buf.at[chip], c_buf)

    next_norm[0] = keep * old_norm + admit * key
    grow = admit * (512.0**-0.5)
    value16 = value.astype(BF16)
    stores = []
    for h in range(4):
        pick = jnp.where(head_row == h, key_raw, 0.0).astype(BF16)
        outer = tn(value16, pick)
        mem[h] = keep[h : h + 1] * mem[h] + grow[h : h + 1] * outer
        stores.append(pltpu.make_async_copy(mem.at[h], next_memory.at[h], out_sem.at[h]))
        stores[h].start()

    table = b_buf[:, 1:2, :].reshape(CHIPS, LANES)
    t0, t1, u0, u1 = (table[:, k : k + 1] for k in range(4))
    below = (iota((CHIPS, CHIPS), 0) > iota((CHIPS, CHIPS), 1)).astype(F32).astype(BF16)
    slot = iota((CHIPS, LANES), 1)
    choose = jnp.where((slot == 4) & (iota((CHIPS, LANES), 0) == chip), 1.0, 0.0)
    weigh = jnp.zeros((CHIPS, LANES), F32)
    for k in range(2):
        eid = (2 * chip + k).astype(F32)
        first, second = t0 == eid, t1 == eid
        hit = jnp.where(first | second, 1.0, 0.0)
        rank = nn(below, jnp.broadcast_to(hit, (CHIPS, LANES)).astype(BF16))
        here = (rank == (slot - 8 * k).astype(F32)) & (slot >= 8 * k) & (slot < 8 * k + 4)
        taken = jnp.where(here, hit, 0.0)
        choose = choose + taken
        weigh = weigh + taken * (jnp.where(first, u0, 0.0) + jnp.where(second, u1, 0.0))
    select = jnp.concatenate([choose, choose], axis=0).T[0:16]
    both = jnp.concatenate(
        [jnp.where(lane < CHIPS, select, 0.0), jnp.where(lane < CHIPS, 0.0, select)], axis=0
    ).astype(BF16)
    slot_tokens = reorder(nn(select[:, :CHIPS].astype(BF16), tok_rows[...]).astype(BF16))
    weigh = weigh[:, :16]
    weigh_hi = weigh.astype(BF16)
    weigh_lo = (weigh - weigh_hi.astype(F32)).astype(BF16)

    whole(2, c_buf).wait_recv()
    rows = jnp.concatenate([p.astype(BF16) for p in gathered(c_buf)], axis=1)
    flat = nt(w_all[4].reshape(32, 2048), jnp.concatenate([rows, rows], axis=0))
    p_buf[chip] = jnp.where(lane < CHIPS, flat[0:16], flat[16:32]).astype(BF16)
    exchange(3, lambda there: p_buf.at[chip], p_buf)

    whole(3, p_buf).wait_recv()
    halves = nt(both, p_buf[...].reshape(CHIPS * TILE, LANES))
    projected = jnp.concatenate([halves[0:16], halves[16:32]], axis=1)
    middle = (slot_tokens + projected).astype(BF16)
    middle32 = middle.astype(F32)
    scale = lax.rsqrt(jnp.mean(middle32 * middle32, axis=-1, keepdims=True) + EPS)
    expert_in = (middle32 * scale * late_gain).astype(BF16).astype(F32)
    e_rows[0] = expert_in[0:8]
    e_rows[1] = expert_in[8:16]

    def to_partner(n, source, target):
        return pltpu.make_async_remote_copy(
            src_ref=source,
            dst_ref=target,
            send_sem=pair_sem.at[0, n],
            recv_sem=pair_sem.at[1, n],
            device_id=(partner,),
            device_id_type=MESH,
        )

    rows_over = to_partner(5, e_rows.at[other], x_rows.at[core])
    rows_over.start()
    x_rows[core] = e_rows[core]
    for load in gate_loads + up_loads + [down_load]:
        load.wait()
    rows_over.wait_recv()
    x = x_rows[...].reshape(16, 2048).astype(BF16)
    result = jnp.zeros((16, 2048), F32)
    for n in range(4):
        span = slice(256 * n, 256 * (n + 1))
        gate_part = nn(x[:, :1024], gate_v[0, :, :, span].reshape(1024, 256)) + nn(
            x[:, 1024:], gate_v[1, :, :, span].reshape(1024, 256)
        )
        up_part = nn(x[:, :1024], up_v[0, :, :, span].reshape(1024, 256)) + nn(
            x[:, 1024:], up_v[1, :, :, span].reshape(1024, 256)
        )
        hidden = (gate_part / (1.0 + jnp.exp(-gate_part)) * up_part).astype(BF16)
        result = result + nn(hidden, down_v[span, :])
    result = result.astype(BF16).astype(F32)
    r_send[0] = result[0:8]
    r_send[1] = result[8:16]
    rows_back = to_partner(6, r_send.at[other], r_rows.at[core])
    rows_back.start()
    r_rows[core] = r_send[core]
    own_middle = restore(middle)[4:5]
    for s, piece in enumerate(pieces(own_middle)):
        tile32[s : s + 1, :] = piece
    rows_back.wait_recv()

    slots = r_rows[...].reshape(16, 2048).astype(BF16)
    mixed = nn(weigh_hi, slots) + nn(weigh_lo, slots)
    for s, piece in enumerate(pieces(mixed)):
        rows32[pl.ds(s, CHIPS, stride=TILE), :] = piece
    f_src[...] = rows32[...].reshape(CHIPS, TILE, LANES).astype(BF16)
    exchange(4, lambda there: f_src.at[there], f_buf)
    f_buf[chip] = f_src[chip]
    whole(4, f_buf).wait_recv()
    total = tile32[...] + jnp.sum(f_buf[...].astype(F32), axis=0)
    final = total.astype(BF16).astype(F32)
    for s in range(TILE):
        out_ref[:, LANES * s : LANES * (s + 1)] = final[s : s + 1].astype(BF16)

    for phase, buf in enumerate((a_buf, b_buf, c_buf, p_buf, f_buf)):
        whole(phase, buf).wait_send()
    for swap in swaps:
        swap.wait_send()
    rows_over.wait_send()
    rows_back.wait_send()
    for store in stores:
        store.wait()


def local(
    tokens,
    mixer_gain,
    query_weight,
    key_weight,
    value_weight,
    outgate_weight,
    input_weight,
    forget_weight,
    forget_bias,
    memory_matrix,
    memory_norm,
    memory_max,
    mixer_out,
    expert_gain,
    expert_gate,
    expert_up,
    expert_down,
    route_group,
    route_member,
    group_weight,
    member_weight,
):
    vmem = pl.BlockSpec(memory_space=pltpu.VMEM)
    smem = pl.BlockSpec(memory_space=pltpu.SMEM)
    hbm = pl.BlockSpec(memory_space=pl.ANY)
    dma = pltpu.SemaphoreType.DMA
    out, matrix, norm, top = pl.pallas_call(
        layer,
        out_shape=(
            jax.ShapeDtypeStruct((1, 2048), BF16),
            jax.ShapeDtypeStruct((4, 512, 512), F32),
            jax.ShapeDtypeStruct((1, 4, 512), F32),
            jax.ShapeDtypeStruct((1, 4), F32),
        ),
        in_specs=[vmem, vmem, hbm, hbm, hbm, hbm, vmem, vmem, smem, hbm, vmem, smem, hbm, vmem, hbm, hbm, hbm, smem, smem, smem, smem],
        out_specs=(vmem, hbm, vmem, vmem),
        scratch_shapes=[
            pltpu.VMEM((5, 2, 16, 2048), BF16),
            pltpu.VMEM((4, 512, 512), F32),
            pltpu.VMEM((4, 512, 512), BF16),
            pltpu.VMEM((2, CHIPS, 16, 1024), BF16),
            pltpu.VMEM((2, CHIPS, 16, 1024), BF16),
            pltpu.VMEM((1024, 2048), BF16),
            pltpu.VMEM((LANES, 2048), BF16),
            pltpu.VMEM((256, 256), BF16),
            pltpu.VMEM((CHIPS * TILE, LANES), F32),
            pltpu.VMEM((CHIPS, 2048), BF16),
            pltpu.VMEM((TILE, LANES), F32),
            pltpu.VMEM((CHIPS, TILE, LANES), BF16),
            pltpu.VMEM((CHIPS, 2, LANES), F32),
            pltpu.VMEM((CHIPS, 2, LANES), F32),
            pltpu.VMEM((CHIPS, TILE, LANES), BF16),
            pltpu.VMEM((CHIPS, TILE, LANES), BF16),
            pltpu.VMEM((CHIPS, TILE, LANES), BF16),
            pltpu.VMEM((CHIPS, TILE, LANES), BF16),
            pltpu.VMEM((2, 8, 2048), F32),
            pltpu.VMEM((2, 8, 2048), F32),
            pltpu.VMEM((2, 8, 2048), F32),
            pltpu.VMEM((2, 8, 2048), F32),
            dma((5,)),
            dma((5,)),
            dma((6,)),
            dma((5,)),
            dma((4,)),
            dma((2, 7)),
        ],
        compiler_params=pltpu.CompilerParams(collective_id=0, has_side_effects=True),
    )(
        tokens,
        mixer_gain.reshape(1, 2048),
        query_weight.T,
        key_weight.T,
        value_weight.T,
        outgate_weight.T,
        input_weight.T,
        forget_weight.T,
        forget_bias,
        memory_matrix.reshape(4, 512, 512),
        memory_norm,
        memory_max,
        mixer_out.T,
        expert_gain.reshape(1, 2048),
        expert_gate.reshape(CHIPS, 2, 16, 1024),
        expert_up.reshape(CHIPS, 2, 16, 1024),
        expert_down.reshape(1024, 2048),
        route_group,
        route_member,
        group_weight,
        member_weight,
    )
    return out, matrix.reshape(1, 4, 512, 512), norm, top


def solution(mesh):
    columns, rows = P(None, "ep"), P("ep", None)
    cube, block = P("ep", None, None), P("ep", None, None, None)
    placed = (
        rows, P(), columns, columns, columns, columns, P(), P(), P(), block, cube, rows, columns, P(), cube, cube, cube,
        P("ep"), rows, P("ep"), rows,
    )
    return jax.shard_map(local, mesh=mesh, in_specs=placed, out_specs=(rows, block, cube, rows), check_vma=False)
```

```python
import functools

import jax
import jax.numpy as jnp
from jax import lax
from jax.experimental import pallas as pl
from jax.experimental.pallas import tpu as pltpu
from jax.sharding import PartitionSpec as P

MESH = pl.DeviceIdType.MESH
F32 = jnp.float32
BF16 = jnp.bfloat16
EPS = 1e-06
CHIPS = 64
TILE = 16
LANES = 128
MEMBERS = 32


def nt(a, b):
    return lax.dot_general(a, b, (((1,), (1,)), ((), ())), preferred_element_type=F32)


def nn(a, b):
    return lax.dot_general(a, b, (((1,), (0,)), ((), ())), preferred_element_type=F32)


def tn(a, b):
    return lax.dot_general(a, b, (((0,), (0,)), ((), ())), preferred_element_type=F32)


def iota(shape, dim):
    return lax.broadcasted_iota(jnp.int32, shape, dim)


def pieces(row):
    return [row[:, LANES * s : LANES * (s + 1)] for s in range(row.shape[1] // LANES)]


def layer(
    tokens_in,
    mixer_gain_in,
    wq,
    wk,
    wv,
    wo,
    wi_in,
    wf_in,
    forget_bias_in,
    memory,
    memory_norm_in,
    memory_max_in,
    wm,
    expert_gain_in,
    gate,
    up,
    down,
    route_member_in,
    member_weight_in,
    route_group,
    group_weight,
    out_ref,
    mem,
    next_norm,
    next_max_ref,
    tokens,
    mixer_gain,
    wi,
    wf,
    memory_norm,
    expert_gain,
    forget_bias,
    memory_max,
    route_member,
    member_weight,
    w_all,
    w_mix,
    mem16,
    gate_v,
    up_v,
    down_v,
    spread,
    rows32,
    tok_rows,
    tile32,
    a_buf,
    b_src,
    b_buf,
    c_buf,
    p_buf,
    f_src,
    f_buf,
    e_rows,
    x_rows,
    r_rows,
    r_send,
    send_sem,
    recv_sem,
    load_sem,
    small_sem,
    w_sem,
    pair_sem,
    line_sem,
):
    me = lax.axis_index("ep")
    core = lax.rem(me, 2)
    chip = lax.div(me, 2)
    other = 1 - core
    partner = me + 1 - 2 * core
    cz, cy, cx = lax.div(chip, 16), lax.rem(lax.div(chip, 4), 4), lax.rem(chip, 4)

    def peer(i):
        dz, dy, dx = lax.div(i, 16), lax.rem(lax.div(i, 4), 4), lax.rem(i, 4)
        there = lax.rem(cz + dz, 4) * 16 + lax.rem(cy + dy, 4) * 4 + lax.rem(cx + dx, 4)
        return there, there * 2 + core

    barrier = pltpu.get_barrier_semaphore()

    def greet(i, carry):
        pl.semaphore_signal(barrier, inc=1, device_id=(peer(i)[1],), device_id_type=MESH)
        return carry

    lax.fori_loop(1, CHIPS, greet, 0)
    pl.semaphore_signal(barrier, inc=1, device_id=(partner,), device_id_type=MESH)

    small = (
        (tokens_in, tokens),
        (mixer_gain_in, mixer_gain),
        (wi_in, wi),
        (wf_in, wf),
        (memory_norm_in, memory_norm),
        (expert_gain_in, expert_gain),
        (forget_bias_in, forget_bias),
        (memory_max_in, memory_max),
        (route_member_in, route_member),
        (member_weight_in, member_weight),
    )
    small_loads = [pltpu.make_async_copy(ref, into, small_sem.at[n]) for n, (ref, into) in enumerate(small)]
    own_loads = [
        pltpu.make_async_copy(ref, w_all.at[j, core], w_sem.at[j]) for j, ref in enumerate((wq, wk, wv, wo))
    ] + [pltpu.make_async_copy(wm, w_mix.at[cx, core], w_sem.at[4])]
    mem_load = pltpu.make_async_copy(memory, mem, load_sem.at[0])
    expert_loads = [
        pltpu.make_async_copy(ref, into, load_sem.at[1 + n])
        for n, (ref, into) in enumerate(((gate, gate_v), (up, up_v), (down, down_v)))
    ]
    for load in small_loads + own_loads + [mem_load] + expert_loads:
        load.start()

    def exchange(phase, source, buf, stride=1, slot=chip):
        def send(n, carry):
            there, device = peer(CHIPS - stride * n)
            pltpu.make_async_remote_copy(
                src_ref=source(there),
                dst_ref=buf.at[slot],
                send_sem=send_sem.at[phase],
                recv_sem=recv_sem.at[phase],
                device_id=(device,),
                device_id_type=MESH,
            ).start()
            return carry

        lax.fori_loop(1, CHIPS // stride, send, 0)

    def whole(phase, buf):
        span = buf.at[pl.ds(0, buf.shape[0] - 1)]
        return pltpu.make_async_remote_copy(
            src_ref=span,
            dst_ref=span,
            send_sem=send_sem.at[phase],
            recv_sem=recv_sem.at[phase],
            device_id=(partner,),
            device_id_type=MESH,
        )

    for load in small_loads:
        load.wait()
    token = tokens[...].astype(F32)
    for s, piece in enumerate(pieces(token)):
        tile32[s : s + 1, :] = piece
    a_buf[chip] = tile32[...].astype(BF16)

    pl.semaphore_wait(barrier, CHIPS)

    exchange(0, lambda there: a_buf.at[chip], a_buf)
    swaps = []
    for j, ref in enumerate((wq, wk, wv, wo, wm)):
        swaps.append(
            pltpu.make_async_remote_copy(
                src_ref=ref,
                dst_ref=w_all.at[j, core] if j < 4 else w_mix.at[cx, core],
                send_sem=pair_sem.at[0, j],
                recv_sem=pair_sem.at[1, j],
                device_id=(partner,),
                device_id_type=MESH,
            )
        )
        swaps[j].start()

    gain = mixer_gain[...]
    scale = lax.rsqrt(jnp.mean(token * token, axis=-1, keepdims=True) + EPS)
    normed = (token * scale * gain).astype(BF16).astype(F32)
    head_of = iota((4, 1), 0)

    def column(read):
        value = jnp.zeros((4, 1), F32)
        for h in range(4):
            value = jnp.where(head_of == h, read(h), value)
        return value

    input_pre = jnp.sum(wi[...].astype(F32) * normed, axis=1, keepdims=True)
    forget_pre = jnp.sum(wf[...].astype(F32) * normed, axis=1, keepdims=True) + column(lambda h: forget_bias[h])
    log_forget = jnp.minimum(forget_pre, 0.0) - jnp.log1p(jnp.exp(-jnp.abs(forget_pre)))
    held = log_forget + column(lambda h: memory_max[0, h])
    next_max = jnp.maximum(held, input_pre)
    keep = jnp.exp(held - next_max)
    admit = jnp.exp(input_pre - next_max)
    next_max_ref[...] = jnp.sum(
        jnp.where(iota((4, 4), 0) == iota((4, 4), 1), jnp.broadcast_to(next_max, (4, 4)), 0.0), axis=0, keepdims=True
    )

    lane = iota((1, LANES), 1)
    e0 = (route_group[0] * MEMBERS + route_member[0, 0]).astype(F32)
    e1 = (route_group[0] * MEMBERS + route_member[0, 1]).astype(F32)
    w0 = group_weight[0] * member_weight[0, 0]
    w1 = group_weight[0] * member_weight[0, 1]
    routing = jnp.where(lane == 0, e0, jnp.where(lane == 1, e1, jnp.where(lane == 2, w0, jnp.where(lane == 3, w1, 0.0))))
    b_src[:, 1:2, :] = jnp.broadcast_to(routing[None], (CHIPS, 1, LANES))

    for j in range(4):
        a, b = iota((LANES, 512), 0), iota((LANES, 512), 1)
        spread[:, 512 * j : 512 * (j + 1)] = (a == 32 * j + lax.rem(b, 32)).astype(F32).astype(BF16)
    mem_load.wait()
    for h in range(4):
        mem16[h] = mem[h].astype(BF16)
    for load in own_loads:
        load.wait()
    for swap in swaps[:4]:
        swap.wait_recv()

    def gathered(buf):
        count = buf.shape[0]
        rows32[0 : count * TILE, :] = buf[...].astype(F32).reshape(count * TILE, LANES)
        return [rows32[pl.ds(s, count, stride=TILE), :] for s in range(TILE)]

    whole(0, a_buf).wait_recv()
    parts = gathered(a_buf)
    tok_rows[...] = jnp.concatenate([p.astype(BF16) for p in parts], axis=1)
    squares = parts[0] * parts[0]
    for p in parts[1:]:
        squares = squares + p * p
    scale = lax.rsqrt(jnp.sum(squares, axis=-1, keepdims=True) * (1.0 / 2048.0) + EPS)
    normed_rows = jnp.concatenate(
        [(p * scale * gain[:, LANES * s : LANES * (s + 1)]).astype(BF16) for s, p in enumerate(parts)], axis=1
    )
    cols = nt(normed_rows, w_all[...].reshape(LANES, 2048)).astype(BF16).astype(F32)
    b_src[:, 0:1, :] = cols.reshape(CHIPS, 1, LANES)
    exchange(1, lambda there: b_src.at[there], b_buf)
    b_buf[chip] = b_src[chip]
    line_sends = [
        pltpu.make_async_remote_copy(
            src_ref=w_mix.at[cx, core],
            dst_ref=w_mix.at[cx, core],
            send_sem=line_sem.at[0, d - 1],
            recv_sem=line_sem.at[1, d - 1],
            device_id=(((chip - cx + lax.rem(cx + d, 4)) * 2 + core),),
            device_id_type=MESH,
        )
        for d in (2, 1, 3)
    ]
    for copy in line_sends:
        copy.start()

    whole(1, b_buf).wait_recv()
    got = b_buf[:, 0:1, :].reshape(CHIPS, LANES).astype(BF16)
    wide = nn(got, spread[...])
    mine = lax.div(lax.rem(iota((CHIPS, 2048), 1), 512), 32) == lax.rem(iota((CHIPS, 2048), 0), 16)
    wide = jnp.where(mine, wide, 0.0).astype(BF16)
    heads = (iota((16, CHIPS), 0) == lax.div(iota((16, CHIPS), 1), 16)).astype(F32).astype(BF16)
    packed = nn(heads, wide)[0:4]
    query, key_raw, value, outgate = (packed[:, 512 * j : 512 * (j + 1)] for j in range(4))
    key = key_raw * (512.0**-0.5)
    score = jnp.sum(key * query, axis=-1, keepdims=True)
    old_norm = memory_norm[0]
    denom = keep * jnp.sum(old_norm * query, axis=-1, keepdims=True) + admit * score
    query16 = query.astype(BF16)
    head_row = iota((4, 512), 0)
    carried = jnp.zeros((4, 512), F32)
    for h in range(4):
        carried = jnp.where(head_row == h, nt(query16, mem16[h]), carried)
    numer = keep * carried + (admit * score) * value
    head_out = numer / jnp.maximum(jnp.abs(denom), jnp.exp(-next_max))
    gated = head_out * jax.nn.sigmoid(outgate)
    for b in range(4):
        tile32[pl.ds(b, 4, stride=4), :] = gated[:, LANES * b : LANES * (b + 1)]
    spot = lax.div(chip, 4)
    c_buf[spot] = tile32[...].astype(BF16)
    exchange(2, lambda there: c_buf.at[spot], c_buf, 4, spot)

    line_shares = []
    for n, copy in enumerate(line_sends):
        copy.wait_recv()
    for n in range(3):
        block = w_mix.at[lax.rem(cx + n + 1, 4), core]
        line_shares.append(
            pltpu.make_async_remote_copy(
                src_ref=block,
                dst_ref=block,
                send_sem=line_sem.at[2, n],
                recv_sem=line_sem.at[3, n],
                device_id=(partner,),
                device_id_type=MESH,
            )
        )
        line_shares[n].start()

    next_norm[0] = keep * old_norm + admit * key
    grow = admit * (512.0**-0.5)
    value16 = value.astype(BF16)
    for h in range(4):
        pick = jnp.where(head_row == h, key_raw, 0.0).astype(BF16)
        outer = tn(value16, pick)
        mem[h] = keep[h : h + 1] * mem[h] + grow[h : h + 1] * outer

    table = b_buf[:, 1:2, :].reshape(CHIPS, LANES)
    t0, t1, u0, u1 = (table[:, k : k + 1] for k in range(4))
    below = (iota((CHIPS, CHIPS), 0) > iota((CHIPS, CHIPS), 1)).astype(F32).astype(BF16)
    slot = iota((CHIPS, LANES), 1)
    choose = jnp.where((slot == 4) & (iota((CHIPS, LANES), 0) == chip), 1.0, 0.0)
    weigh = jnp.zeros((CHIPS, LANES), F32)
    for k in range(2):
        eid = (2 * chip + k).astype(F32)
        first, second = t0 == eid, t1 == eid
        hit = jnp.where(first | second, 1.0, 0.0)
        rank = nn(below, jnp.broadcast_to(hit, (CHIPS, LANES)).astype(BF16))
        here = (rank == (slot - 8 * k).astype(F32)) & (slot >= 8 * k) & (slot < 8 * k + 4)
        taken = jnp.where(here, hit, 0.0)
        choose = choose + taken
        weigh = weigh + taken * (jnp.where(first, u0, 0.0) + jnp.where(second, u1, 0.0))
    select = jnp.concatenate([choose, choose], axis=0).T[0:16, 0:CHIPS].astype(BF16)
    slot_tokens = nn(select, tok_rows[...])
    a, b = iota((CHIPS, CHIPS), 0), iota((CHIPS, CHIPS), 1)
    by_line = (b == lax.rem(a, 4) * 16 + lax.div(a, 4)).astype(F32).astype(BF16)
    select_line = nn(select, by_line).astype(BF16)
    weigh = weigh[:, :16]
    weigh_hi = weigh.astype(BF16)
    weigh_lo = (weigh - weigh_hi.astype(F32)).astype(BF16)

    whole(2, c_buf).wait_recv()
    rows = jnp.concatenate([p.astype(BF16) for p in gathered(c_buf)], axis=1)
    swaps[4].wait_recv()
    for copy in line_shares:
        copy.wait_recv()
    p_buf[chip] = nt(rows, w_mix[...].reshape(LANES, 2048)).astype(BF16)
    exchange(3, lambda there: p_buf.at[chip], p_buf)

    whole(3, p_buf).wait_recv()
    wide = jnp.concatenate([p_buf[4 * n : 4 * (n + 1)].reshape(CHIPS, LANES) for n in range(16)], axis=1)
    projected = nn(select_line, wide)
    middle = (slot_tokens + projected).astype(BF16)
    middle32 = middle.astype(F32)
    scale = lax.rsqrt(jnp.mean(middle32 * middle32, axis=-1, keepdims=True) + EPS)
    expert_in = (middle32 * scale * expert_gain[...]).astype(BF16).astype(F32)
    e_rows[0] = expert_in[0:8]
    e_rows[1] = expert_in[8:16]

    def to_partner(n, source, target):
        return pltpu.make_async_remote_copy(
            src_ref=source,
            dst_ref=target,
            send_sem=pair_sem.at[0, n],
            recv_sem=pair_sem.at[1, n],
            device_id=(partner,),
            device_id_type=MESH,
        )

    rows_over = to_partner(5, e_rows.at[other], x_rows.at[core])
    rows_over.start()
    x_rows[core] = e_rows[core]
    for load in expert_loads:
        load.wait()
    rows_over.wait_recv()
    x = x_rows[...].reshape(16, 2048).astype(BF16)
    result = jnp.zeros((16, 2048), F32)
    for n in range(4):
        span = slice(256 * n, 256 * (n + 1))
        gate_part = nn(x, gate_v[:, span])
        up_part = nn(x, up_v[:, span])
        hidden = (gate_part / (1.0 + jnp.exp(-gate_part)) * up_part).astype(BF16)
        result = result + nn(hidden, down_v[span, :])
    result = result.astype(BF16).astype(F32)
    r_send[0] = result[0:8]
    r_send[1] = result[8:16]
    rows_back = to_partner(6, r_send.at[other], r_rows.at[core])
    rows_back.start()
    r_rows[core] = r_send[core]
    own_middle = middle32[4:5]
    for s, piece in enumerate(pieces(own_middle)):
        tile32[s : s + 1, :] = piece
    rows_back.wait_recv()

    slots = r_rows[...].reshape(16, 2048).astype(BF16)
    mixed = nn(weigh_hi, slots) + nn(weigh_lo, slots)
    for s, piece in enumerate(pieces(mixed)):
        rows32[pl.ds(s, CHIPS, stride=TILE), :] = piece
    f_src[...] = rows32[...].reshape(CHIPS, TILE, LANES).astype(BF16)
    exchange(4, lambda there: f_src.at[there], f_buf)
    f_buf[chip] = f_src[chip]
    whole(4, f_buf).wait_recv()
    total = tile32[...] + jnp.sum(f_buf[...].astype(F32), axis=0)
    final = total.astype(BF16).astype(F32)
    for s in range(TILE):
        out_ref[:, LANES * s : LANES * (s + 1)] = final[s : s + 1].astype(BF16)

    for phase, buf in enumerate((a_buf, b_buf, c_buf, p_buf, f_buf)):
        whole(phase, buf).wait_send()
    for copy in swaps + line_sends + line_shares + [rows_over, rows_back]:
        copy.wait_send()


def finish(out_in, mem_in, norm_in, top_in, out, matrix, norm, top, sem):
    stores = [pltpu.make_async_copy(mem_in.at[h], matrix.at[h], sem.at[h]) for h in range(4)]
    for store in stores:
        store.start()
    out[...] = out_in[...]
    norm[...] = norm_in[...]
    top[...] = top_in[...]
    for store in stores:
        store.wait()


def local(
    tokens,
    mixer_gain,
    query_weight,
    key_weight,
    value_weight,
    outgate_weight,
    input_weight,
    forget_weight,
    forget_bias,
    memory_matrix,
    memory_norm,
    memory_max,
    mixer_out,
    expert_gain,
    expert_gate,
    expert_up,
    expert_down,
    route_group,
    route_member,
    group_weight,
    member_weight,
):
    smem = pl.BlockSpec(memory_space=pltpu.SMEM)
    vmem = pl.BlockSpec(memory_space=pltpu.VMEM)
    hbm = pl.BlockSpec(memory_space=pltpu.HBM)
    dma = pltpu.SemaphoreType.DMA
    sizes = ((1, 2048), BF16), ((4, 512, 512), F32), ((1, 4, 512), F32), ((1, 4), F32)
    raw = pl.pallas_call(
        layer,
        out_shape=tuple(pltpu.VMEM(*size) for size in sizes),
        in_specs=[hbm] * 19 + [smem] * 2,
        out_specs=(vmem,) * 4,
        scratch_shapes=[
            pltpu.VMEM((1, 2048), BF16),
            pltpu.VMEM((1, 2048), F32),
            pltpu.VMEM((4, 2048), BF16),
            pltpu.VMEM((4, 2048), BF16),
            pltpu.VMEM((1, 4, 512), F32),
            pltpu.VMEM((1, 2048), F32),
            pltpu.SMEM((4,), F32),
            pltpu.SMEM((1, 4), F32),
            pltpu.SMEM((1, 2), jnp.int32),
            pltpu.SMEM((1, 2), F32),
            pltpu.VMEM((4, 2, 16, 2048), BF16),
            pltpu.VMEM((4, 2, 16, 2048), BF16),
            pltpu.VMEM((4, 512, 512), BF16),
            pltpu.VMEM((2048, 1024), BF16),
            pltpu.VMEM((2048, 1024), BF16),
            pltpu.VMEM((1024, 2048), BF16),
            pltpu.VMEM((LANES, 2048), BF16),
            pltpu.VMEM((CHIPS * TILE, LANES), F32),
            pltpu.VMEM((CHIPS, 2048), BF16),
            pltpu.VMEM((TILE, LANES), F32),
            pltpu.VMEM((CHIPS, TILE, LANES), BF16),
            pltpu.VMEM((CHIPS, 2, LANES), F32),
            pltpu.VMEM((CHIPS, 2, LANES), F32),
            pltpu.VMEM((CHIPS // 4, TILE, LANES), BF16),
            pltpu.VMEM((CHIPS, TILE, LANES), BF16),
            pltpu.VMEM((CHIPS, TILE, LANES), BF16),
            pltpu.VMEM((CHIPS, TILE, LANES), BF16),
            pltpu.VMEM((2, 8, 2048), F32),
            pltpu.VMEM((2, 8, 2048), F32),
            pltpu.VMEM((2, 8, 2048), F32),
            pltpu.VMEM((2, 8, 2048), F32),
            dma((5,)),
            dma((5,)),
            dma((4,)),
            dma((10,)),
            dma((5,)),
            dma((2, 7)),
            dma((4, 3)),
        ],
        compiler_params=pltpu.CompilerParams(
            collective_id=0, has_side_effects=True, vmem_limit_bytes=40 * 1024 * 1024
        ),
    )(
        *(pltpu.with_memory_space_constraint(value, pltpu.HBM) for value in (
        tokens,
        mixer_gain.reshape(1, 2048),
        query_weight.T,
        key_weight.T,
        value_weight.T,
        outgate_weight.T,
        input_weight.T,
        forget_weight.T,
        forget_bias,
        memory_matrix.reshape(4, 512, 512),
        memory_norm,
        memory_max,
        mixer_out.T,
        expert_gain.reshape(1, 2048),
        expert_gate.reshape(2048, 1024),
        expert_up.reshape(2048, 1024),
        expert_down.reshape(1024, 2048),
        route_member,
        member_weight,
        )),
        route_group,
        group_weight,
    )
    out, matrix, norm, top = pl.pallas_call(
        finish,
        out_shape=tuple(jax.ShapeDtypeStruct(*size) for size in sizes),
        in_specs=[vmem] * 4,
        out_specs=(vmem, hbm, vmem, vmem),
        scratch_shapes=[dma((4,))],
        compiler_params=pltpu.CompilerParams(vmem_limit_bytes=8 * 1024 * 1024),
    )(*(pltpu.with_memory_space_constraint(value, pltpu.VMEM) for value in raw))
    return out, matrix.reshape(1, 4, 512, 512), norm, top


def solution(mesh):
    columns, rows = P(None, "ep"), P("ep", None)
    cube, block = P("ep", None, None), P("ep", None, None, None)
    placed = (
        rows, P(), columns, columns, columns, columns, P(), P(), P(), block, cube, rows, columns, P(), cube, cube, cube,
        P("ep"), rows, P("ep"), rows,
    )
    return jax.shard_map(local, mesh=mesh, in_specs=placed, out_specs=(rows, block, cube, rows), check_vma=False)
```

```python
import functools

import jax
import jax.numpy as jnp
from jax import lax
from jax.experimental import pallas as pl
from jax.experimental.pallas import tpu as pltpu
from jax.sharding import PartitionSpec as P

MESH = pl.DeviceIdType.MESH
F32 = jnp.float32
BF16 = jnp.bfloat16
EPS = 1e-06
CHIPS = 64
TILE = 16
LANES = 128
MEMBERS = 32


def nt(a, b):
    return lax.dot_general(a, b, (((1,), (1,)), ((), ())), preferred_element_type=F32)


def nn(a, b):
    return lax.dot_general(a, b, (((1,), (0,)), ((), ())), preferred_element_type=F32)


def tn(a, b):
    return lax.dot_general(a, b, (((0,), (0,)), ((), ())), preferred_element_type=F32)


def iota(shape, dim):
    return lax.broadcasted_iota(jnp.int32, shape, dim)


def pieces(row):
    return [row[:, LANES * s : LANES * (s + 1)] for s in range(row.shape[1] // LANES)]


def layer(
    tokens_in,
    mixer_gain_in,
    wq,
    wk,
    wv,
    wo,
    wi_in,
    wf_in,
    forget_bias_in,
    memory,
    memory_norm_in,
    memory_max_in,
    wm,
    expert_gain_in,
    gate,
    up,
    down,
    route_member_in,
    member_weight_in,
    route_group,
    group_weight,
    out_ref,
    mem,
    next_norm,
    next_max_ref,
    tokens,
    mixer_gain,
    wi,
    wf,
    memory_norm,
    expert_gain,
    forget_bias,
    memory_max,
    route_member,
    member_weight,
    w_all,
    w_mix,
    mem16,
    gate_v,
    up_v,
    down_v,
    spread,
    rows32,
    tok_rows,
    tile32,
    a_buf,
    b_src,
    b_buf,
    c_buf,
    p_buf,
    f_src,
    f_buf,
    e_rows,
    x_rows,
    r_rows,
    r_send,
    send_sem,
    recv_sem,
    load_sem,
    small_sem,
    w_sem,
    pair_sem,
    line_sem,
):
    me = lax.axis_index("ep")
    core = lax.rem(me, 2)
    chip = lax.div(me, 2)
    other = 1 - core
    partner = me + 1 - 2 * core
    cz, cy, cx = lax.div(chip, 16), lax.rem(lax.div(chip, 4), 4), lax.rem(chip, 4)

    steps = [tuple(lax.rem(at + d, 4) * size for d in range(4)) for at, size in ((cz, 16), (cy, 4), (cx, 1))]
    offsets = [(dz, dy, dx) for dz in range(4) for dy in range(4) for dx in range(4)][1:]
    offsets.sort(key=lambda offset: -sum(min(d, 4 - d) for d in offset))

    def peer(offset):
        there = steps[0][offset[0]] + steps[1][offset[1]] + steps[2][offset[2]]
        return there, there * 2 + core

    barrier = pltpu.get_barrier_semaphore()

    for offset in offsets:
        pl.semaphore_signal(barrier, inc=1, device_id=(peer(offset)[1],), device_id_type=MESH)
    pl.semaphore_signal(barrier, inc=1, device_id=(partner,), device_id_type=MESH)

    small = (
        (tokens_in, tokens),
        (mixer_gain_in, mixer_gain),
        (wi_in, wi),
        (wf_in, wf),
        (memory_norm_in, memory_norm),
        (expert_gain_in, expert_gain),
        (forget_bias_in, forget_bias),
        (memory_max_in, memory_max),
        (route_member_in, route_member),
        (member_weight_in, member_weight),
    )
    small_loads = [pltpu.make_async_copy(ref, into, small_sem.at[n]) for n, (ref, into) in enumerate(small)]
    own_loads = [
        pltpu.make_async_copy(ref, w_all.at[j, core], w_sem.at[j]) for j, ref in enumerate((wq, wk, wv, wo))
    ] + [pltpu.make_async_copy(wm, w_mix.at[cx, core], w_sem.at[4])]
    mem_load = pltpu.make_async_copy(memory, mem, load_sem.at[0])
    expert_loads = [
        pltpu.make_async_copy(ref, into, load_sem.at[1 + n])
        for n, (ref, into) in enumerate(((gate, gate_v), (up, up_v), (down, down_v)))
    ]
    for load in small_loads + own_loads + [mem_load] + expert_loads:
        load.start()

    def exchange(phase, source, buf, across=True, slot=chip):
        for offset in offsets:
            if offset[2] and not across:
                continue
            there, device = peer(offset)
            pltpu.make_async_remote_copy(
                src_ref=source(there),
                dst_ref=buf.at[slot],
                send_sem=send_sem.at[phase],
                recv_sem=recv_sem.at[phase],
                device_id=(device,),
                device_id_type=MESH,
            ).start()

    def whole(phase, buf):
        span = buf.at[pl.ds(0, buf.shape[0] - 1)]
        return pltpu.make_async_remote_copy(
            src_ref=span,
            dst_ref=span,
            send_sem=send_sem.at[phase],
            recv_sem=recv_sem.at[phase],
            device_id=(partner,),
            device_id_type=MESH,
        )

    for load in small_loads:
        load.wait()
    token = tokens[...].astype(F32)
    for s, piece in enumerate(pieces(token)):
        tile32[s : s + 1, :] = piece
    a_buf[chip] = tile32[...].astype(BF16)

    pl.semaphore_wait(barrier, CHIPS)

    exchange(0, lambda there: a_buf.at[chip], a_buf)
    swaps = []
    for j, ref in enumerate((wq, wk, wv, wo, wm)):
        swaps.append(
            pltpu.make_async_remote_copy(
                src_ref=ref,
                dst_ref=w_all.at[j, core] if j < 4 else w_mix.at[cx, core],
                send_sem=pair_sem.at[0, j],
                recv_sem=pair_sem.at[1, j],
                device_id=(partner,),
                device_id_type=MESH,
            )
        )
        swaps[j].start()

    gain = mixer_gain[...]
    scale = lax.rsqrt(jnp.mean(token * token, axis=-1, keepdims=True) + EPS)
    normed = (token * scale * gain).astype(BF16).astype(F32)
    head_of = iota((4, 1), 0)

    def column(read):
        value = jnp.zeros((4, 1), F32)
        for h in range(4):
            value = jnp.where(head_of == h, read(h), value)
        return value

    input_pre = jnp.sum(wi[...].astype(F32) * normed, axis=1, keepdims=True)
    forget_pre = jnp.sum(wf[...].astype(F32) * normed, axis=1, keepdims=True) + column(lambda h: forget_bias[h])
    log_forget = jnp.minimum(forget_pre, 0.0) - jnp.log1p(jnp.exp(-jnp.abs(forget_pre)))
    held = log_forget + column(lambda h: memory_max[0, h])
    next_max = jnp.maximum(held, input_pre)
    keep = jnp.exp(held - next_max)
    admit = jnp.exp(input_pre - next_max)
    next_max_ref[...] = jnp.sum(
        jnp.where(iota((4, 4), 0) == iota((4, 4), 1), jnp.broadcast_to(next_max, (4, 4)), 0.0), axis=0, keepdims=True
    )

    lane = iota((1, LANES), 1)
    e0 = (route_group[0] * MEMBERS + route_member[0, 0]).astype(F32)
    e1 = (route_group[0] * MEMBERS + route_member[0, 1]).astype(F32)
    w0 = group_weight[0] * member_weight[0, 0]
    w1 = group_weight[0] * member_weight[0, 1]
    routing = jnp.where(lane == 0, e0, jnp.where(lane == 1, e1, jnp.where(lane == 2, w0, jnp.where(lane == 3, w1, 0.0))))
    b_src[:, 1:2, :] = jnp.broadcast_to(routing[None], (CHIPS, 1, LANES))

    for j in range(4):
        a, b = iota((LANES, 512), 0), iota((LANES, 512), 1)
        spread[:, 512 * j : 512 * (j + 1)] = (a == 32 * j + lax.rem(b, 32)).astype(F32).astype(BF16)
    mem_load.wait()
    for h in range(4):
        mem16[h] = mem[h].astype(BF16)
    for load in own_loads:
        load.wait()
    for swap in swaps[:4]:
        swap.wait_recv()

    def gathered(buf):
        count = buf.shape[0]
        rows32[0 : count * TILE, :] = buf[...].astype(F32).reshape(count * TILE, LANES)
        return [rows32[pl.ds(s, count, stride=TILE), :] for s in range(TILE)]

    whole(0, a_buf).wait_recv()
    parts = gathered(a_buf)
    tok_rows[...] = jnp.concatenate([p.astype(BF16) for p in parts], axis=1)
    squares = parts[0] * parts[0]
    for p in parts[1:]:
        squares = squares + p * p
    scale = lax.rsqrt(jnp.sum(squares, axis=-1, keepdims=True) * (1.0 / 2048.0) + EPS)
    normed_rows = jnp.concatenate(
        [(p * scale * gain[:, LANES * s : LANES * (s + 1)]).astype(BF16) for s, p in enumerate(parts)], axis=1
    )
    cols = nt(normed_rows, w_all[...].reshape(LANES, 2048)).astype(BF16).astype(F32)
    b_src[:, 0:1, :] = cols.reshape(CHIPS, 1, LANES)
    exchange(1, lambda there: b_src.at[there], b_buf)
    b_buf[chip] = b_src[chip]
    line_sends = [
        pltpu.make_async_remote_copy(
            src_ref=w_mix.at[cx, core],
            dst_ref=w_mix.at[cx, core],
            send_sem=line_sem.at[0, d - 1],
            recv_sem=line_sem.at[1, d - 1],
            device_id=(((chip - cx + lax.rem(cx + d, 4)) * 2 + core),),
            device_id_type=MESH,
        )
        for d in (2, 1, 3)
    ]
    for copy in line_sends:
        copy.start()

    whole(1, b_buf).wait_recv()
    got = b_buf[:, 0:1, :].reshape(CHIPS, LANES).astype(BF16)
    wide = nn(got, spread[...])
    mine = lax.div(lax.rem(iota((CHIPS, 2048), 1), 512), 32) == lax.rem(iota((CHIPS, 2048), 0), 16)
    wide = jnp.where(mine, wide, 0.0).astype(BF16)
    heads = (iota((16, CHIPS), 0) == lax.div(iota((16, CHIPS), 1), 16)).astype(F32).astype(BF16)
    packed = nn(heads, wide)[0:4]
    query, key_raw, value, outgate = (packed[:, 512 * j : 512 * (j + 1)] for j in range(4))
    key = key_raw * (512.0**-0.5)
    score = jnp.sum(key * query, axis=-1, keepdims=True)
    old_norm = memory_norm[0]
    denom = keep * jnp.sum(old_norm * query, axis=-1, keepdims=True) + admit * score
    query16 = query.astype(BF16)
    head_row = iota((4, 512), 0)
    carried = jnp.zeros((4, 512), F32)
    for h in range(4):
        carried = jnp.where(head_row == h, nt(query16, mem16[h]), carried)
    numer = keep * carried + (admit * score) * value
    head_out = numer / jnp.maximum(jnp.abs(denom), jnp.exp(-next_max))
    gated = head_out * jax.nn.sigmoid(outgate)
    for b in range(4):
        tile32[pl.ds(b, 4, stride=4), :] = gated[:, LANES * b : LANES * (b + 1)]
    spot = lax.div(chip, 4)
    c_buf[spot] = tile32[...].astype(BF16)
    exchange(2, lambda there: c_buf.at[spot], c_buf, False, spot)

    line_shares = []
    for n, copy in enumerate(line_sends):
        copy.wait_recv()
    for n in range(3):
        block = w_mix.at[lax.rem(cx + n + 1, 4), core]
        line_shares.append(
            pltpu.make_async_remote_copy(
                src_ref=block,
                dst_ref=block,
                send_sem=line_sem.at[2, n],
                recv_sem=line_sem.at[3, n],
                device_id=(partner,),
                device_id_type=MESH,
            )
        )
        line_shares[n].start()

    next_norm[0] = keep * old_norm + admit * key
    grow = admit * (512.0**-0.5)
    value16 = value.astype(BF16)
    for h in range(4):
        pick = jnp.where(head_row == h, key_raw, 0.0).astype(BF16)
        outer = tn(value16, pick)
        mem[h] = keep[h : h + 1] * mem[h] + grow[h : h + 1] * outer

    table = b_buf[:, 1:2, :].reshape(CHIPS, LANES)
    t0, t1, u0, u1 = (table[:, k : k + 1] for k in range(4))
    below = (iota((CHIPS, CHIPS), 0) > iota((CHIPS, CHIPS), 1)).astype(F32).astype(BF16)
    slot = iota((CHIPS, LANES), 1)
    choose = jnp.where((slot == 4) & (iota((CHIPS, LANES), 0) == chip), 1.0, 0.0)
    weigh = jnp.zeros((CHIPS, LANES), F32)
    for k in range(2):
        eid = (2 * chip + k).astype(F32)
        first, second = t0 == eid, t1 == eid
        hit = jnp.where(first | second, 1.0, 0.0)
        rank = nn(below, jnp.broadcast_to(hit, (CHIPS, LANES)).astype(BF16))
        here = (rank == (slot - 8 * k).astype(F32)) & (slot >= 8 * k) & (slot < 8 * k + 4)
        taken = jnp.where(here, hit, 0.0)
        choose = choose + taken
        weigh = weigh + taken * (jnp.where(first, u0, 0.0) + jnp.where(second, u1, 0.0))
    select = jnp.concatenate([choose, choose], axis=0).T[0:16, 0:CHIPS].astype(BF16)
    slot_tokens = nn(select, tok_rows[...])
    a, b = iota((CHIPS, CHIPS), 0), iota((CHIPS, CHIPS), 1)
    by_line = (b == lax.rem(a, 4) * 16 + lax.div(a, 4)).astype(F32).astype(BF16)
    select_line = nn(select, by_line).astype(BF16)
    weigh = weigh[:, :16]
    weigh_hi = weigh.astype(BF16)
    weigh_lo = (weigh - weigh_hi.astype(F32)).astype(BF16)

    whole(2, c_buf).wait_recv()
    rows = jnp.concatenate([p.astype(BF16) for p in gathered(c_buf)], axis=1)
    swaps[4].wait_recv()
    for copy in line_shares:
        copy.wait_recv()
    p_buf[chip] = nt(rows, w_mix[...].reshape(LANES, 2048)).astype(BF16)
    exchange(3, lambda there: p_buf.at[chip], p_buf)

    whole(3, p_buf).wait_recv()
    wide = jnp.concatenate([p_buf[4 * n : 4 * (n + 1)].reshape(CHIPS, LANES) for n in range(16)], axis=1)
    projected = nn(select_line, wide)
    middle = (slot_tokens + projected).astype(BF16)
    middle32 = middle.astype(F32)
    scale = lax.rsqrt(jnp.mean(middle32 * middle32, axis=-1, keepdims=True) + EPS)
    expert_in = (middle32 * scale * expert_gain[...]).astype(BF16).astype(F32)
    e_rows[0] = expert_in[0:8]
    e_rows[1] = expert_in[8:16]

    def to_partner(n, source, target):
        return pltpu.make_async_remote_copy(
            src_ref=source,
            dst_ref=target,
            send_sem=pair_sem.at[0, n],
            recv_sem=pair_sem.at[1, n],
            device_id=(partner,),
            device_id_type=MESH,
        )

    rows_over = to_partner(5, e_rows.at[other], x_rows.at[core])
    rows_over.start()
    x_rows[core] = e_rows[core]
    for load in expert_loads:
        load.wait()
    rows_over.wait_recv()
    x = x_rows[...].reshape(16, 2048).astype(BF16)
    gate_part = nn(x, gate_v[...])
    up_part = nn(x, up_v[...])
    hidden = (gate_part / (1.0 + jnp.exp(-gate_part)) * up_part).astype(BF16)
    result = nn(hidden, down_v[...])
    result = result.astype(BF16).astype(F32)
    r_send[0] = result[0:8]
    r_send[1] = result[8:16]
    rows_back = to_partner(6, r_send.at[other], r_rows.at[core])
    rows_back.start()
    r_rows[core] = r_send[core]
    own_middle = middle32[4:5]
    for s, piece in enumerate(pieces(own_middle)):
        tile32[s : s + 1, :] = piece
    rows_back.wait_recv()

    slots = r_rows[...].reshape(16, 2048).astype(BF16)
    mixed = nn(weigh_hi, slots) + nn(weigh_lo, slots)
    for s, piece in enumerate(pieces(mixed)):
        rows32[pl.ds(s, CHIPS, stride=TILE), :] = piece
    f_src[...] = rows32[...].reshape(CHIPS, TILE, LANES).astype(BF16)
    exchange(4, lambda there: f_src.at[there], f_buf)
    f_buf[chip] = f_src[chip]
    whole(4, f_buf).wait_recv()
    total = tile32[...] + jnp.sum(f_buf[...].astype(F32), axis=0)
    final = total.astype(BF16).astype(F32)
    for s in range(TILE):
        out_ref[:, LANES * s : LANES * (s + 1)] = final[s : s + 1].astype(BF16)

    for phase, buf in enumerate((a_buf, b_buf, c_buf, p_buf, f_buf)):
        whole(phase, buf).wait_send()
    for copy in swaps + line_sends + line_shares + [rows_over, rows_back]:
        copy.wait_send()


def finish(out_in, mem_in, norm_in, top_in, out, matrix, norm, top, sem):
    copies = [
        pltpu.make_async_copy(mem_in.at[h, pl.ds(256 * n, 256)], matrix.at[h, pl.ds(256 * n, 256)], sem.at[2 * h + n])
        for h in range(4)
        for n in range(2)
    ]
    for n, (source, target) in enumerate(((out_in, out), (norm_in, norm), (top_in, top))):
        copies.append(pltpu.make_async_copy(source, target, sem.at[8 + n]))
    for copy in copies:
        copy.start()
    for copy in copies:
        copy.wait()


def local(
    tokens,
    mixer_gain,
    query_weight,
    key_weight,
    value_weight,
    outgate_weight,
    input_weight,
    forget_weight,
    forget_bias,
    memory_matrix,
    memory_norm,
    memory_max,
    mixer_out,
    expert_gain,
    expert_gate,
    expert_up,
    expert_down,
    route_group,
    route_member,
    group_weight,
    member_weight,
):
    smem = pl.BlockSpec(memory_space=pltpu.SMEM)
    vmem = pl.BlockSpec(memory_space=pltpu.VMEM)
    hbm = pl.BlockSpec(memory_space=pltpu.HBM)
    dma = pltpu.SemaphoreType.DMA
    sizes = ((1, 2048), BF16), ((4, 512, 512), F32), ((1, 4, 512), F32), ((1, 4), F32)
    raw = pl.pallas_call(
        layer,
        out_shape=tuple(pltpu.VMEM(*size) for size in sizes),
        in_specs=[hbm] * 19 + [smem] * 2,
        out_specs=(vmem,) * 4,
        scratch_shapes=[
            pltpu.VMEM((1, 2048), BF16),
            pltpu.VMEM((1, 2048), F32),
            pltpu.VMEM((4, 2048), BF16),
            pltpu.VMEM((4, 2048), BF16),
            pltpu.VMEM((1, 4, 512), F32),
            pltpu.VMEM((1, 2048), F32),
            pltpu.SMEM((4,), F32),
            pltpu.SMEM((1, 4), F32),
            pltpu.SMEM((1, 2), jnp.int32),
            pltpu.SMEM((1, 2), F32),
            pltpu.VMEM((4, 2, 16, 2048), BF16),
            pltpu.VMEM((4, 2, 16, 2048), BF16),
            pltpu.VMEM((4, 512, 512), BF16),
            pltpu.VMEM((2048, 1024), BF16),
            pltpu.VMEM((2048, 1024), BF16),
            pltpu.VMEM((1024, 2048), BF16),
            pltpu.VMEM((LANES, 2048), BF16),
            pltpu.VMEM((CHIPS * TILE, LANES), F32),
            pltpu.VMEM((CHIPS, 2048), BF16),
            pltpu.VMEM((TILE, LANES), F32),
            pltpu.VMEM((CHIPS, TILE, LANES), BF16),
            pltpu.VMEM((CHIPS, 2, LANES), F32),
            pltpu.VMEM((CHIPS, 2, LANES), F32),
            pltpu.VMEM((CHIPS // 4, TILE, LANES), BF16),
            pltpu.VMEM((CHIPS, TILE, LANES), BF16),
            pltpu.VMEM((CHIPS, TILE, LANES), BF16),
            pltpu.VMEM((CHIPS, TILE, LANES), BF16),
            pltpu.VMEM((2, 8, 2048), F32),
            pltpu.VMEM((2, 8, 2048), F32),
            pltpu.VMEM((2, 8, 2048), F32),
            pltpu.VMEM((2, 8, 2048), F32),
            dma((5,)),
            dma((5,)),
            dma((4,)),
            dma((10,)),
            dma((5,)),
            dma((2, 7)),
            dma((4, 3)),
        ],
        compiler_params=pltpu.CompilerParams(
            collective_id=0, has_side_effects=True, vmem_limit_bytes=40 * 1024 * 1024
        ),
    )(
        *(pltpu.with_memory_space_constraint(value, pltpu.HBM) for value in (
        tokens,
        mixer_gain.reshape(1, 2048),
        query_weight.T,
        key_weight.T,
        value_weight.T,
        outgate_weight.T,
        input_weight.T,
        forget_weight.T,
        forget_bias,
        memory_matrix.reshape(4, 512, 512),
        memory_norm,
        memory_max,
        mixer_out.T,
        expert_gain.reshape(1, 2048),
        expert_gate.reshape(2048, 1024),
        expert_up.reshape(2048, 1024),
        expert_down.reshape(1024, 2048),
        route_member,
        member_weight,
        )),
        route_group,
        group_weight,
    )
    out, matrix, norm, top = pl.pallas_call(
        finish,
        out_shape=tuple(jax.ShapeDtypeStruct(*size) for size in sizes),
        in_specs=[vmem] * 4,
        out_specs=(hbm,) * 4,
        scratch_shapes=[dma((11,))],
        compiler_params=pltpu.CompilerParams(vmem_limit_bytes=8 * 1024 * 1024),
    )(*(pltpu.with_memory_space_constraint(value, pltpu.VMEM) for value in raw))
    return out, matrix.reshape(1, 4, 512, 512), norm, top


def solution(mesh):
    columns, rows = P(None, "ep"), P("ep", None)
    cube, block = P("ep", None, None), P("ep", None, None, None)
    placed = (
        rows, P(), columns, columns, columns, columns, P(), P(), P(), block, cube, rows, columns, P(), cube, cube, cube,
        P("ep"), rows, P("ep"), rows,
    )
    return jax.shard_map(local, mesh=mesh, in_specs=placed, out_specs=(rows, block, cube, rows), check_vma=False)
```

```python
import functools

import jax
import jax.numpy as jnp
from jax import lax
from jax.experimental import pallas as pl
from jax.experimental.pallas import tpu as pltpu
from jax.sharding import PartitionSpec as P

MESH = pl.DeviceIdType.MESH
F32 = jnp.float32
BF16 = jnp.bfloat16
EPS = 1e-06
CHIPS = 64
TILE = 16
LANES = 128
MEMBERS = 32


def nt(a, b):
    return lax.dot_general(a, b, (((1,), (1,)), ((), ())), preferred_element_type=F32)


def nn(a, b):
    return lax.dot_general(a, b, (((1,), (0,)), ((), ())), preferred_element_type=F32)


def tn(a, b):
    return lax.dot_general(a, b, (((0,), (0,)), ((), ())), preferred_element_type=F32)


def iota(shape, dim):
    return lax.broadcasted_iota(jnp.int32, shape, dim)


def pieces(row):
    return [row[:, LANES * s : LANES * (s + 1)] for s in range(row.shape[1] // LANES)]


def layer(
    tokens_in,
    mixer_gain_in,
    wq,
    wk,
    wv,
    wo,
    wi_in,
    wf_in,
    forget_bias_in,
    memory,
    memory_norm_in,
    memory_max_in,
    wm,
    expert_gain_in,
    gate,
    up,
    down,
    route_member_in,
    member_weight_in,
    route_group,
    group_weight,
    out_ref,
    mem,
    next_norm,
    next_max_ref,
    tokens,
    mixer_gain,
    wi,
    wf,
    memory_norm,
    expert_gain,
    forget_bias,
    memory_max,
    route_member,
    member_weight,
    w_all,
    w_mix,
    mem16,
    gate_v,
    up_v,
    down_v,
    spread,
    rows32,
    tok_rows,
    tile32,
    a_buf,
    b_src,
    b_buf,
    c_buf,
    p_buf,
    f_src,
    f_buf,
    e_rows,
    x_rows,
    r_rows,
    r_send,
    send_sem,
    recv_sem,
    load_sem,
    small_sem,
    w_sem,
    pair_sem,
    line_sem,
):
    me = lax.axis_index("ep")
    core = lax.rem(me, 2)
    chip = lax.div(me, 2)
    other = 1 - core
    partner = me + 1 - 2 * core
    cz, cy, cx = lax.div(chip, 16), lax.rem(lax.div(chip, 4), 4), lax.rem(chip, 4)

    steps = [tuple(lax.rem(at + d, 4) * size for d in range(4)) for at, size in ((cz, 16), (cy, 4), (cx, 1))]
    offsets = [(dz, dy, dx) for dz in range(4) for dy in range(4) for dx in range(4)][1:]
    offsets.sort(key=lambda offset: -sum(min(d, 4 - d) for d in offset))
    offsets.sort(key=lambda offset: -sum(min(d, 4 - d) for d in offset[:2]))

    def peer(offset):
        there = steps[0][offset[0]] + steps[1][offset[1]] + steps[2][offset[2]]
        return there, there * 2 + core

    barrier = pltpu.get_barrier_semaphore()

    for offset in offsets:
        pl.semaphore_signal(barrier, inc=1, device_id=(peer(offset)[1],), device_id_type=MESH)
    pl.semaphore_signal(barrier, inc=1, device_id=(partner,), device_id_type=MESH)

    small = (
        (tokens_in, tokens),
        (mixer_gain_in, mixer_gain),
        (wi_in, wi),
        (wf_in, wf),
        (memory_norm_in, memory_norm),
        (expert_gain_in, expert_gain),
        (forget_bias_in, forget_bias),
        (memory_max_in, memory_max),
        (route_member_in, route_member),
        (member_weight_in, member_weight),
    )
    small_loads = [pltpu.make_async_copy(ref, into, small_sem.at[n]) for n, (ref, into) in enumerate(small)]
    own_loads = [
        pltpu.make_async_copy(ref, w_all.at[j, core], w_sem.at[j]) for j, ref in enumerate((wq, wk, wv, wo))
    ] + [pltpu.make_async_copy(wm, w_mix.at[cx, core], w_sem.at[4])]
    mem_load = pltpu.make_async_copy(memory, mem, load_sem.at[0])
    expert_loads = [
        pltpu.make_async_copy(ref, into, load_sem.at[1 + n])
        for n, (ref, into) in enumerate(((gate, gate_v), (up, up_v), (down, down_v)))
    ]
    for load in small_loads + own_loads + [mem_load] + expert_loads:
        load.start()

    def exchange(phase, source, buf, across=True, slot=chip):
        for offset in offsets:
            if offset[2] and not across:
                continue
            there, device = peer(offset)
            pltpu.make_async_remote_copy(
                src_ref=source(there),
                dst_ref=buf.at[slot],
                send_sem=send_sem.at[phase],
                recv_sem=recv_sem.at[phase],
                device_id=(device,),
                device_id_type=MESH,
            ).start()

    def whole(phase, buf):
        span = buf.at[pl.ds(0, buf.shape[0] - 1)]
        return pltpu.make_async_remote_copy(
            src_ref=span,
            dst_ref=span,
            send_sem=send_sem.at[phase],
            recv_sem=recv_sem.at[phase],
            device_id=(partner,),
            device_id_type=MESH,
        )

    for load in small_loads:
        load.wait()
    token = tokens[...].astype(F32)
    for s, piece in enumerate(pieces(token)):
        tile32[s : s + 1, :] = piece
    a_buf[chip] = tile32[...].astype(BF16)

    pl.semaphore_wait(barrier, CHIPS)

    exchange(0, lambda there: a_buf.at[chip], a_buf)
    swaps = []
    for j, ref in enumerate((wq, wk, wv, wo, wm)):
        swaps.append(
            pltpu.make_async_remote_copy(
                src_ref=ref,
                dst_ref=w_all.at[j, core] if j < 4 else w_mix.at[cx, core],
                send_sem=pair_sem.at[0, j],
                recv_sem=pair_sem.at[1, j],
                device_id=(partner,),
                device_id_type=MESH,
            )
        )
        swaps[j].start()

    gain = mixer_gain[...]
    scale = lax.rsqrt(jnp.mean(token * token, axis=-1, keepdims=True) + EPS)
    normed = (token * scale * gain).astype(BF16).astype(F32)
    head_of = iota((4, 1), 0)

    def column(read):
        value = jnp.zeros((4, 1), F32)
        for h in range(4):
            value = jnp.where(head_of == h, read(h), value)
        return value

    input_pre = jnp.sum(wi[...].astype(F32) * normed, axis=1, keepdims=True)
    forget_pre = jnp.sum(wf[...].astype(F32) * normed, axis=1, keepdims=True) + column(lambda h: forget_bias[h])
    log_forget = jnp.minimum(forget_pre, 0.0) - jnp.log1p(jnp.exp(-jnp.abs(forget_pre)))
    held = log_forget + column(lambda h: memory_max[0, h])
    next_max = jnp.maximum(held, input_pre)
    keep = jnp.exp(held - next_max)
    admit = jnp.exp(input_pre - next_max)
    next_max_ref[...] = jnp.sum(
        jnp.where(iota((4, 4), 0) == iota((4, 4), 1), jnp.broadcast_to(next_max, (4, 4)), 0.0), axis=0, keepdims=True
    )

    lane = iota((1, LANES), 1)
    e0 = (route_group[0] * MEMBERS + route_member[0, 0]).astype(F32)
    e1 = (route_group[0] * MEMBERS + route_member[0, 1]).astype(F32)
    w0 = group_weight[0] * member_weight[0, 0]
    w1 = group_weight[0] * member_weight[0, 1]
    routing = jnp.where(lane == 0, e0, jnp.where(lane == 1, e1, jnp.where(lane == 2, w0, jnp.where(lane == 3, w1, 0.0))))
    b_src[:, 1:2, :] = jnp.broadcast_to(routing[None], (CHIPS, 1, LANES))

    for j in range(4):
        a, b = iota((LANES, 512), 0), iota((LANES, 512), 1)
        spread[:, 512 * j : 512 * (j + 1)] = (a == 32 * j + lax.rem(b, 32)).astype(F32).astype(BF16)
    mem_load.wait()
    for h in range(4):
        mem16[h] = mem[h].astype(BF16)
    for load in own_loads:
        load.wait()
    for swap in swaps[:4]:
        swap.wait_recv()

    def gathered(buf):
        count = buf.shape[0]
        rows32[0 : count * TILE, :] = buf[...].astype(F32).reshape(count * TILE, LANES)
        return [rows32[pl.ds(s, count, stride=TILE), :] for s in range(TILE)]

    whole(0, a_buf).wait_recv()
    parts = gathered(a_buf)
    tok_rows[...] = jnp.concatenate([p.astype(BF16) for p in parts], axis=1)
    squares = parts[0] * parts[0]
    for p in parts[1:]:
        squares = squares + p * p
    scale = lax.rsqrt(jnp.sum(squares, axis=-1, keepdims=True) * (1.0 / 2048.0) + EPS)
    normed_rows = jnp.concatenate(
        [(p * scale * gain[:, LANES * s : LANES * (s + 1)]).astype(BF16) for s, p in enumerate(parts)], axis=1
    )
    cols = nt(normed_rows, w_all[...].reshape(LANES, 2048)).astype(BF16).astype(F32)
    b_src[:, 0:1, :] = cols.reshape(CHIPS, 1, LANES)
    exchange(1, lambda there: b_src.at[there], b_buf)
    b_buf[chip] = b_src[chip]
    line_sends = [
        pltpu.make_async_remote_copy(
            src_ref=w_mix.at[cx, core],
            dst_ref=w_mix.at[cx, core],
            send_sem=line_sem.at[0, d - 1],
            recv_sem=line_sem.at[1, d - 1],
            device_id=(((chip - cx + lax.rem(cx + d, 4)) * 2 + core),),
            device_id_type=MESH,
        )
        for d in (2, 1, 3)
    ]
    for copy in line_sends:
        copy.start()

    whole(1, b_buf).wait_recv()
    got = b_buf[:, 0:1, :].reshape(CHIPS, LANES).astype(BF16)
    wide = nn(got, spread[...])
    mine = lax.div(lax.rem(iota((CHIPS, 2048), 1), 512), 32) == lax.rem(iota((CHIPS, 2048), 0), 16)
    wide = jnp.where(mine, wide, 0.0).astype(BF16)
    heads = (iota((16, CHIPS), 0) == lax.div(iota((16, CHIPS), 1), 16)).astype(F32).astype(BF16)
    packed = nn(heads, wide)[0:4]
    query, key_raw, value, outgate = (packed[:, 512 * j : 512 * (j + 1)] for j in range(4))
    key = key_raw * (512.0**-0.5)
    score = jnp.sum(key * query, axis=-1, keepdims=True)
    old_norm = memory_norm[0]
    denom = keep * jnp.sum(old_norm * query, axis=-1, keepdims=True) + admit * score
    query16 = query.astype(BF16)
    head_row = iota((4, 512), 0)
    carried = jnp.zeros((4, 512), F32)
    for h in range(4):
        carried = jnp.where(head_row == h, nt(query16, mem16[h]), carried)
    numer = keep * carried + (admit * score) * value
    head_out = numer / jnp.maximum(jnp.abs(denom), jnp.exp(-next_max))
    gated = head_out * jax.nn.sigmoid(outgate)
    for b in range(4):
        tile32[pl.ds(b, 4, stride=4), :] = gated[:, LANES * b : LANES * (b + 1)]
    spot = lax.div(chip, 4)
    c_buf[spot] = tile32[...].astype(BF16)
    exchange(2, lambda there: c_buf.at[spot], c_buf, False, spot)

    line_shares = []
    for n, copy in enumerate(line_sends):
        copy.wait_recv()
    for n in range(3):
        block = w_mix.at[lax.rem(cx + n + 1, 4), core]
        line_shares.append(
            pltpu.make_async_remote_copy(
                src_ref=block,
                dst_ref=block,
                send_sem=line_sem.at[2, n],
                recv_sem=line_sem.at[3, n],
                device_id=(partner,),
                device_id_type=MESH,
            )
        )
        line_shares[n].start()

    next_norm[0] = keep * old_norm + admit * key
    grow = admit * (512.0**-0.5)
    value16 = value.astype(BF16)
    for h in range(4):
        pick = jnp.where(head_row == h, key_raw, 0.0).astype(BF16)
        outer = tn(value16, pick)
        mem[h] = keep[h : h + 1] * mem[h] + grow[h : h + 1] * outer

    table = b_buf[:, 1:2, :].reshape(CHIPS, LANES)
    t0, t1, u0, u1 = (table[:, k : k + 1] for k in range(4))
    below = (iota((CHIPS, CHIPS), 0) > iota((CHIPS, CHIPS), 1)).astype(F32).astype(BF16)
    slot = iota((CHIPS, LANES), 1)
    choose = jnp.where((slot == 4) & (iota((CHIPS, LANES), 0) == chip), 1.0, 0.0)
    weigh = jnp.zeros((CHIPS, LANES), F32)
    for k in range(2):
        eid = (2 * chip + k).astype(F32)
        first, second = t0 == eid, t1 == eid
        hit = jnp.where(first | second, 1.0, 0.0)
        rank = nn(below, jnp.broadcast_to(hit, (CHIPS, LANES)).astype(BF16))
        here = (rank == (slot - 8 * k).astype(F32)) & (slot >= 8 * k) & (slot < 8 * k + 4)
        taken = jnp.where(here, hit, 0.0)
        choose = choose + taken
        weigh = weigh + taken * (jnp.where(first, u0, 0.0) + jnp.where(second, u1, 0.0))
    select = jnp.concatenate([choose, choose], axis=0).T[0:16, 0:CHIPS].astype(BF16)
    slot_tokens = nn(select, tok_rows[...])
    a, b = iota((CHIPS, CHIPS), 0), iota((CHIPS, CHIPS), 1)
    by_line = (b == lax.rem(a, 4) * 16 + lax.div(a, 4)).astype(F32).astype(BF16)
    select_line = nn(select, by_line).astype(BF16)
    weigh = weigh[:, :16]
    weigh_hi = weigh.astype(BF16).astype(F32)
    weights = jnp.concatenate([weigh_hi, weigh - weigh_hi], axis=1).astype(BF16)

    whole(2, c_buf).wait_recv()
    rows = jnp.concatenate([p.astype(BF16) for p in gathered(c_buf)], axis=1)
    swaps[4].wait_recv()
    for copy in line_shares:
        copy.wait_recv()
    p_buf[chip] = nt(rows, w_mix[...].reshape(LANES, 2048)).astype(BF16)
    exchange(3, lambda there: p_buf.at[chip], p_buf)

    whole(3, p_buf).wait_recv()
    wide = jnp.concatenate([p_buf[4 * n : 4 * (n + 1)].reshape(CHIPS, LANES) for n in range(16)], axis=1)
    projected = nn(select_line, wide)
    middle = (slot_tokens + projected).astype(BF16)
    middle32 = middle.astype(F32)
    scale = lax.rsqrt(jnp.mean(middle32 * middle32, axis=-1, keepdims=True) + EPS)
    expert_in = (middle32 * scale * expert_gain[...]).astype(BF16).astype(F32)
    e_rows[0] = expert_in[0:8]
    e_rows[1] = expert_in[8:16]

    def to_partner(n, source, target):
        return pltpu.make_async_remote_copy(
            src_ref=source,
            dst_ref=target,
            send_sem=pair_sem.at[0, n],
            recv_sem=pair_sem.at[1, n],
            device_id=(partner,),
            device_id_type=MESH,
        )

    rows_over = to_partner(5, e_rows.at[other], x_rows.at[core])
    rows_over.start()
    x_rows[core] = e_rows[core]
    for load in expert_loads:
        load.wait()
    rows_over.wait_recv()
    x = x_rows[...].reshape(16, 2048).astype(BF16)
    gate_part = nn(x, gate_v[...])
    up_part = nn(x, up_v[...])
    hidden = (gate_part / (1.0 + jnp.exp(-gate_part)) * up_part).astype(BF16)
    result = nn(hidden, down_v[...])
    result = result.astype(BF16).astype(F32)
    r_send[0] = result[0:8]
    r_send[1] = result[8:16]
    rows_back = to_partner(6, r_send.at[other], r_rows.at[core])
    rows_back.start()
    r_rows[core] = r_send[core]
    own_middle = middle32[4:5]
    for s, piece in enumerate(pieces(own_middle)):
        tile32[s : s + 1, :] = piece
    rows_back.wait_recv()

    slots = r_rows[...].reshape(16, 2048).astype(BF16)
    slots = jnp.concatenate([slots, slots], axis=0)
    for n in range(8):
        mixed = nn(weights, slots[:, 256 * n : 256 * (n + 1)])
        for s, piece in enumerate(pieces(mixed)):
            rows32[pl.ds(2 * n + s, CHIPS, stride=TILE), :] = piece
    f_src[...] = rows32[...].reshape(CHIPS, TILE, LANES).astype(BF16)
    exchange(4, lambda there: f_src.at[there], f_buf)
    f_buf[chip] = f_src[chip]
    for phase, buf in enumerate((a_buf, b_buf, c_buf, p_buf)):
        whole(phase, buf).wait_send()
    for copy in swaps + line_sends + line_shares + [rows_over, rows_back]:
        copy.wait_send()
    whole(4, f_buf).wait_recv()
    total = tile32[...] + jnp.sum(f_buf[...].astype(F32), axis=0)
    final = total.astype(BF16).astype(F32)
    for s in range(TILE):
        out_ref[:, LANES * s : LANES * (s + 1)] = final[s : s + 1].astype(BF16)
    whole(4, f_buf).wait_send()


def finish(out_in, mem_in, norm_in, top_in, out, matrix, norm, top, sem):
    copies = [
        pltpu.make_async_copy(mem_in.at[h, pl.ds(256 * n, 256)], matrix.at[h, pl.ds(256 * n, 256)], sem.at[2 * h + n])
        for h in range(4)
        for n in range(2)
    ]
    for n, (source, target) in enumerate(((out_in, out), (norm_in, norm), (top_in, top))):
        copies.append(pltpu.make_async_copy(source, target, sem.at[8 + n]))
    for copy in copies:
        copy.start()
    for copy in copies:
        copy.wait()


def local(
    tokens,
    mixer_gain,
    query_weight,
    key_weight,
    value_weight,
    outgate_weight,
    input_weight,
    forget_weight,
    forget_bias,
    memory_matrix,
    memory_norm,
    memory_max,
    mixer_out,
    expert_gain,
    expert_gate,
    expert_up,
    expert_down,
    route_group,
    route_member,
    group_weight,
    member_weight,
):
    smem = pl.BlockSpec(memory_space=pltpu.SMEM)
    vmem = pl.BlockSpec(memory_space=pltpu.VMEM)
    hbm = pl.BlockSpec(memory_space=pltpu.HBM)
    dma = pltpu.SemaphoreType.DMA
    sizes = ((1, 2048), BF16), ((4, 512, 512), F32), ((1, 4, 512), F32), ((1, 4), F32)
    raw = pl.pallas_call(
        layer,
        out_shape=tuple(pltpu.VMEM(*size) for size in sizes),
        in_specs=[hbm] * 19 + [smem] * 2,
        out_specs=(vmem,) * 4,
        scratch_shapes=[
            pltpu.VMEM((1, 2048), BF16),
            pltpu.VMEM((1, 2048), F32),
            pltpu.VMEM((4, 2048), BF16),
            pltpu.VMEM((4, 2048), BF16),
            pltpu.VMEM((1, 4, 512), F32),
            pltpu.VMEM((1, 2048), F32),
            pltpu.SMEM((4,), F32),
            pltpu.SMEM((1, 4), F32),
            pltpu.SMEM((1, 2), jnp.int32),
            pltpu.SMEM((1, 2), F32),
            pltpu.VMEM((4, 2, 16, 2048), BF16),
            pltpu.VMEM((4, 2, 16, 2048), BF16),
            pltpu.VMEM((4, 512, 512), BF16),
            pltpu.VMEM((2048, 1024), BF16),
            pltpu.VMEM((2048, 1024), BF16),
            pltpu.VMEM((1024, 2048), BF16),
            pltpu.VMEM((LANES, 2048), BF16),
            pltpu.VMEM((CHIPS * TILE, LANES), F32),
            pltpu.VMEM((CHIPS, 2048), BF16),
            pltpu.VMEM((TILE, LANES), F32),
            pltpu.VMEM((CHIPS, TILE, LANES), BF16),
            pltpu.VMEM((CHIPS, 2, LANES), F32),
            pltpu.VMEM((CHIPS, 2, LANES), F32),
            pltpu.VMEM((CHIPS // 4, TILE, LANES), BF16),
            pltpu.VMEM((CHIPS, TILE, LANES), BF16),
            pltpu.VMEM((CHIPS, TILE, LANES), BF16),
            pltpu.VMEM((CHIPS, TILE, LANES), BF16),
            pltpu.VMEM((2, 8, 2048), F32),
            pltpu.VMEM((2, 8, 2048), F32),
            pltpu.VMEM((2, 8, 2048), F32),
            pltpu.VMEM((2, 8, 2048), F32),
            dma((5,)),
            dma((5,)),
            dma((4,)),
            dma((10,)),
            dma((5,)),
            dma((2, 7)),
            dma((4, 3)),
        ],
        compiler_params=pltpu.CompilerParams(
            collective_id=0, has_side_effects=True, vmem_limit_bytes=40 * 1024 * 1024
        ),
    )(
        *(pltpu.with_memory_space_constraint(value, pltpu.HBM) for value in (
        tokens,
        mixer_gain.reshape(1, 2048),
        query_weight.T,
        key_weight.T,
        value_weight.T,
        outgate_weight.T,
        input_weight.T,
        forget_weight.T,
        forget_bias,
        memory_matrix.reshape(4, 512, 512),
        memory_norm,
        memory_max,
        mixer_out.T,
        expert_gain.reshape(1, 2048),
        expert_gate.reshape(2048, 1024),
        expert_up.reshape(2048, 1024),
        expert_down.reshape(1024, 2048),
        route_member,
        member_weight,
        )),
        route_group,
        group_weight,
    )
    out, matrix, norm, top = pl.pallas_call(
        finish,
        out_shape=tuple(jax.ShapeDtypeStruct(*size) for size in sizes),
        in_specs=[vmem] * 4,
        out_specs=(hbm,) * 4,
        scratch_shapes=[dma((11,))],
        compiler_params=pltpu.CompilerParams(vmem_limit_bytes=8 * 1024 * 1024),
    )(*(pltpu.with_memory_space_constraint(value, pltpu.VMEM) for value in raw))
    return out, matrix.reshape(1, 4, 512, 512), norm, top


def solution(mesh):
    columns, rows = P(None, "ep"), P("ep", None)
    cube, block = P("ep", None, None), P("ep", None, None, None)
    placed = (
        rows, P(), columns, columns, columns, columns, P(), P(), P(), block, cube, rows, columns, P(), cube, cube, cube,
        P("ep"), rows, P("ep"), rows,
    )
    return jax.shard_map(local, mesh=mesh, in_specs=placed, out_specs=(rows, block, cube, rows), check_vma=False)
```
